512 devices in a mesh: sp: 64 (over z, y), tp: 8 (over x, core).
Axes of the slice: x: 4, y: 8, z: 8, core: 2. Of those that a mesh axis runs over, the one named last changes fastest.
Arguments:
- latent: bfloat16 [32768, 2048], P(('sp', 'tp')), may hold values from -6 to 6
- context: bfloat16 [1024, 2048], P('sp'), may hold values from -6 to 6
- condition: float32 [2048], replicated, may hold values from -6 to 6
- context_condition: float32 [2048], replicated, may hold values from -6 to 6
- modulation_weight: bfloat16 [2048, 3, 2048], P('sp', None, 'tp'), may hold values from -0.125 to 0.125
- norm_gain: float32 [2048], replicated, may hold values from 0.1 to 1.9
- query_weight: bfloat16 [2048, 2048], P(None, 'tp'), may hold values from -0.125 to 0.125
- key_weight: bfloat16 [2048, 2048], P(None, 'tp'), may hold values from -0.125 to 0.125
- value_weight: bfloat16 [2048, 2048], P(None, 'tp'), may hold values from -0.125 to 0.125
- log_decay: float32 [2, 32], P(None, 'tp')
- head_gain: float32 [2048], P('tp'), may hold values from 0.1 to 1.9
- output_weight: bfloat16 [2048, 2048], P('sp'), may hold values from -0.125 to 0.125
Outputs:
- output: bfloat16 [32768, 2048], P(('sp', 'tp'))
The draws below stay inside these ranges and needn't reach their ends.
All inputs are finite; a program needn't handle non-finite values.
Results may differ from the reference program's by a relative error of at most 0.0065.
Values may be sent and summed in bfloat16 or wider, within the bound.
A program may use at most 128 MiB of HBM per device.

```python
import jax
import jax.numpy as jnp
from jax import lax

D = 2048
HEADS = 32
HEAD = 64
BLOCK = 128
CTX = 1024
TOK_DEV = 512
TOKENS = 32768


def draw_log_decay(key, part):
    decays = []
    for direction in range(2):
        branch_key = jax.random.fold_in(key, 37 + direction)
        order_key, fast_key, slow_key, middle_key = jax.random.split(branch_key, 4)
        ranking = jax.random.permutation(order_key, HEADS)
        fast_count = max(1, HEADS // 4)
        middle_count = max(1, HEADS // 4)
        fast_spread = jax.random.uniform(fast_key, (HEADS,), jnp.float32)
        slow_spread = jax.random.uniform(slow_key, (HEADS,), jnp.float32)
        middle_spread = jax.random.uniform(middle_key, (HEADS,), jnp.float32, jnp.log(0.1), jnp.log(4.0))
        fast_rate = -1.0 / (BLOCK * (0.25 + 0.5 * fast_spread))
        middle_rate = -jnp.exp(middle_spread) / TOK_DEV
        slow_rate = jnp.log(0.1) * (0.2 + 0.8 * slow_spread) / TOKENS
        chosen = jnp.where(ranking < fast_count, fast_rate, jnp.where(ranking < fast_count + middle_count, middle_rate, slow_rate))
        decays.append(chosen)
    return jnp.stack(decays).astype(jnp.float32)


def level_of(key, dims, cuts, low, largest):
    factor_of, own = 1.0, jax.random.fold_in(key, 6)
    for position, blocks in cuts:
        draws = jnp.exp(jax.random.uniform(jax.random.fold_in(own, position), (blocks,), jnp.float32, low / len(cuts), largest / len(cuts)))
        factor_of = factor_of * jnp.repeat(draws, dims[position] // blocks).reshape([-1 if axis == position else 1 for axis in range(len(dims))])
    return factor_of


def scatter_about(rng, shape, scale, limit, cuts=(), kind=jnp.bfloat16):
    values = scale * jax.random.normal(rng, shape, jnp.float32)
    if cuts:
        values = values * level_of(rng, shape, cuts, -0.22, 0.18)
    return jnp.clip(values, -limit, limit).astype(kind)


def setup_inputs(seed: int = 0) -> dict:
    key_of = jax.random.split(jax.random.key(seed), 13)
    return {
        "latent": scatter_about(key_of[0], (TOKENS, D), 1.0, 6.0, ((0, 512),)),
        "context": scatter_about(key_of[1], (CTX, D), 1.0, 6.0, ((0, 64),)),
        "condition": scatter_about(key_of[2], (D,), 1.0, 6.0, (), jnp.float32),
        "context_condition": scatter_about(key_of[3], (D,), 1.0, 6.0, (), jnp.float32),
        "modulation_weight": scatter_about(key_of[4], (D, 3, D), D ** -0.5, 0.125, ((0, 64), (2, 8))),
        "norm_gain": jnp.clip(1.0 + 0.18 * jax.random.normal(key_of[5], (D,), jnp.float32), 0.1, 1.9),
        "query_weight": scatter_about(key_of[6], (D, HEADS * HEAD), D ** -0.5, 0.125, ((1, 8),)),
        "key_weight": scatter_about(key_of[7], (D, HEADS * HEAD), D ** -0.5, 0.125, ((1, 8),)),
        "value_weight": scatter_about(key_of[8], (D, HEADS * HEAD), D ** -0.5, 0.125, ((1, 8),)),
        "log_decay": draw_log_decay(jax.random.fold_in(key_of[12], 71), 0),
        "head_gain": jnp.clip(1.0 + 0.18 * jax.random.normal(key_of[10], (HEADS * HEAD,), jnp.float32), 0.1, 1.9),
        "output_weight": scatter_about(key_of[11], (HEADS * HEAD, D), (HEADS * HEAD) ** -0.5, 0.125, ((0, 64),)),
    }


EPSILON = 1e-06
ROTARY_BASE = 10000.0
MAXIMAL_ACCURACY = lax.Precision.HIGHEST

def rotation_tables(positions):
    half_size = HEAD // 2
    frequency = 1.0 / ROTARY_BASE ** jnp.linspace(0.0, 1.0, half_size, dtype=jnp.float32)
    angles = positions[:, None] * frequency[None, :]
    return (jnp.cos(angles), jnp.sin(angles))

def rotate(projected, positions):
    cos_table, sin_table = rotation_tables(positions)
    half_size = HEAD // 2
    lower_half = projected[..., :half_size]
    upper_half = projected[..., half_size:]
    cos_table = cos_table[:, None, :]
    sin_table = sin_table[:, None, :]
    return jnp.concatenate([lower_half * cos_table - upper_half * sin_table, lower_half * sin_table + upper_half * cos_table], axis=-1)

def modulated(rows, gain, shift, scale):
    widened = rows.astype(jnp.float32)
    scaled = widened * lax.rsqrt(lax.optimization_barrier(jnp.mean(widened * widened, axis=-1, keepdims=True)) + EPSILON)
    return (scaled * gain * (1.0 + scale) + shift).astype(jnp.bfloat16)

def project(rows, weight):
    return jnp.dot(rows, weight, preferred_element_type=jnp.float32).reshape(rows.shape[0], HEADS, HEAD)

def sweep(queries, keys, values, log_rate, start_state):
    length = queries.shape[0]
    blocks = length // BLOCK
    offsets = jnp.arange(BLOCK, dtype=jnp.float32)
    distance = offsets[:, None] - offsets[None, :]
    decay_mask = jnp.where(distance >= 0, jnp.exp(log_rate[:, None, None] * jnp.maximum(distance, 0.0)[None]), 0.0)
    query_decay = jnp.exp(log_rate[:, None] * (offsets + 1.0)[None]).T
    key_decay = jnp.exp(log_rate[:, None] * (BLOCK - 1.0 - offsets)[None]).T
    block_decay = jnp.exp(log_rate * BLOCK)
    query_blocks = queries.reshape(blocks, BLOCK, HEADS, HEAD)
    key_blocks = keys.reshape(blocks, BLOCK, HEADS, HEAD)
    value_blocks = values.reshape(blocks, BLOCK, HEADS, HEAD)

    def block_step(state, pieces):
        broad_query_matrix = pieces[0].astype(jnp.float32)
        broad_key_matrix = pieces[1].astype(jnp.float32)
        broad_value_matrix = pieces[2].astype(jnp.float32)
        affinity_scores = jnp.einsum('nsg,psg->snp', broad_query_matrix, broad_key_matrix, precision=MAXIMAL_ACCURACY)
        weight_tensors = lax.optimization_barrier((affinity_scores * decay_mask).astype(jnp.bfloat16)).astype(jnp.float32)
        inside_block = jnp.einsum('ngj,jnr->gnr', weight_tensors, broad_value_matrix, precision=MAXIMAL_ACCURACY)
        carried = jnp.einsum('lhd,hde->lhe', broad_query_matrix, state, precision=MAXIMAL_ACCURACY) * query_decay[:, :, None]
        update = jnp.einsum('lhd,lhe->hde', broad_key_matrix * key_decay[:, :, None], broad_value_matrix, precision=MAXIMAL_ACCURACY)
        return (block_decay[:, None, None] * state + update, inside_block + carried)
    final_state, outputs = lax.scan(block_step, start_state, (query_blocks, key_blocks, value_blocks))
    return outputs.reshape(length, HEADS, HEAD)

def reference(latent, context, condition, context_condition, modulation_weight, norm_gain, query_weight, key_weight, value_weight, log_decay, head_gain, output_weight):
    activated = jax.nn.silu(jnp.stack([condition, context_condition])).astype(jnp.bfloat16)
    modulation = jnp.dot(activated, modulation_weight.reshape(D, 3 * D), preferred_element_type=jnp.float32).reshape(2, 3, D)
    normed = modulated(latent, norm_gain, modulation[0, 0], modulation[0, 1])
    context_normed = modulated(context, norm_gain, modulation[1, 0], modulation[1, 1])
    latent_positions = CTX + jnp.arange(TOKENS, dtype=jnp.float32)
    context_positions = jnp.arange(CTX, dtype=jnp.float32)
    queries = (rotate(project(normed, query_weight), latent_positions) * HEAD ** (-0.5)).astype(jnp.bfloat16)
    keys = rotate(project(normed, key_weight), latent_positions).astype(jnp.bfloat16)
    values = project(normed, value_weight).astype(jnp.bfloat16)
    context_keys = rotate(project(context_normed, key_weight), context_positions).astype(jnp.bfloat16)
    context_values = project(context_normed, value_weight).astype(jnp.bfloat16)
    broad_key_matrix = context_keys.astype(jnp.float32)
    broad_value_matrix = context_values.astype(jnp.float32)
    forward_weight = jnp.exp(log_decay[0][None, :] * (CTX - 1.0 - context_positions)[:, None])
    backward_weight = jnp.exp(log_decay[1][None, :] * context_positions[:, None])
    start_forward = jnp.einsum('jhd,jhe->hde', broad_key_matrix * forward_weight[:, :, None], broad_value_matrix, precision=MAXIMAL_ACCURACY)
    start_backward = jnp.einsum('jhd,jhe->hde', broad_key_matrix * backward_weight[:, :, None], broad_value_matrix, precision=MAXIMAL_ACCURACY)
    forward = sweep(queries, keys, values, log_decay[0], start_forward)
    backward = jnp.flip(sweep(jnp.flip(queries, 0), jnp.flip(keys, 0), jnp.flip(values, 0), log_decay[1], start_backward), 0)
    combined = forward + backward
    centre = lax.optimization_barrier(jnp.mean(combined, axis=-1, keepdims=True))
    spread = lax.optimization_barrier(jnp.mean(jnp.square(combined - centre), axis=-1, keepdims=True))
    retained = ((combined - centre) * lax.rsqrt(spread + EPSILON) * head_gain.reshape(HEADS, HEAD)).astype(jnp.bfloat16)
    retained = retained.reshape(TOKENS, HEADS * HEAD)
    mixed = jnp.dot(retained, output_weight, preferred_element_type=jnp.float32)
    return (latent.astype(jnp.float32) + modulation[0, 2] * mixed).astype(jnp.bfloat16)
```

```python
import functools

import jax
import jax.numpy as jnp
import numpy as np
from jax import lax
from jax.experimental import pallas as pl
from jax.experimental.pallas import tpu as pltpu
from jax.sharding import Mesh
from jax.sharding import PartitionSpec as P

HEAD = 64
HALF = HEAD // 2
BLOCK = 128
SP = ("sp_0", "sp_1")
TP = ("tp_0", "tp_1")
SP_TP = SP + TP
EPSILON = 1e-06
ROTARY_BASE = 10000.0
F32, BF16 = jnp.float32, jnp.bfloat16
MESH = pl.DeviceIdType.MESH
VMEM_LIMIT = 60 * 1024 * 1024


def remote(src, dst, send_sem, recv_sem, device):
    return pltpu.make_async_remote_copy(
        src_ref=src, dst_ref=dst, send_sem=send_sem, recv_sem=recv_sem,
        device_id=device, device_id_type=MESH,
    )


def place():
    return {a: lax.axis_index(a) for a in SP_TP}


def tp_peers(at, nx):
    core, x = at["tp_1"], at["tp_0"]
    peers = [{"tp_0": x, "tp_1": 1 - core}]
    for k in range(1, nx):
        there = lax.rem(x + k, nx)
        peers += [{"tp_0": there, "tp_1": core}, {"tp_0": there, "tp_1": 1 - core}]
    return peers


def line_peers(at, axis, n):
    return [{axis: lax.rem(at[axis] + k, n)} for k in range(1, n)]


def greet(peers):
    barrier = pltpu.get_barrier_semaphore()
    for peer in peers:
        pl.semaphore_signal(barrier, inc=1, device_id=peer, device_id_type=MESH)
    pl.semaphore_wait(barrier, len(peers))


class Line:
    def __init__(self, at, axis, n, send_sems, recv_sems):
        self.me, self.axis, self.n = at[axis], axis, n
        self.send_sems, self.recv_sems = send_sems, recv_sems
        self.sent = []

    def start(self, source_of, slots):
        for k in range(1, self.n):
            there = lax.rem(self.me + k, self.n)
            copy = remote(
                source_of(there), slots.at[self.me], self.send_sems.at[k],
                self.recv_sems.at[self.me], {self.axis: there},
            )
            copy.start()
            self.sent.append(copy)

    def wait(self, slots):
        for k in range(1, self.n):
            source = lax.rem(self.me + self.n - k, self.n)
            remote(
                slots.at[source], slots.at[source], self.send_sems.at[k],
                self.recv_sems.at[source], {self.axis: source},
            ).wait_recv()

    def drain(self):
        for copy in self.sent:
            copy.wait_send()


class Gather:
    def __init__(self, at, nx, rows, slot, sems):
        self.x, self.core, self.nx, self.rows, self.slot = at["tp_0"], at["tp_1"], nx, rows, slot
        self.send_sems, self.recv_sems = sems
        self.half = rows // 2
        self.sent = []

    def index(self, steps):
        return lax.rem(self.x + self.nx + steps, self.nx)

    def put(self, src, x_of, core_of, first, count, sem, device):
        copy = remote(
            src, self.slot(x_of * 2 + core_of, first, count), self.send_sems.at[sem],
            self.recv_sems.at[sem], device,
        )
        copy.start()
        self.sent.append(copy)

    def came(self, x_of, core_of, first, count, sem):
        view = self.slot(x_of * 2 + core_of, first, count)
        remote(view, view, self.send_sems.at[sem], self.recv_sems.at[sem], {"tp_0": self.x}).wait_recv()

    def start(self, own):
        x, core, h = self.x, self.core, self.half
        right, left = {"tp_0": self.index(1)}, {"tp_0": self.index(-1)}
        self.put(own(0, h), x, core, 0, h, 0, right)
        self.put(own(h, h), x, core, h, h, 2, left)
        self.put(own(h, h), x, core, h, h, 1, right)
        self.put(own(0, h), x, core, 0, h, 3, left)
        self.put(own(0, self.rows), x, core, 0, self.rows, 6, {"tp_1": 1 - core})

    def forward(self):
        core, h = self.core, self.half
        left, right, over = self.index(-1), self.index(1), {"tp_1": 1 - core}
        self.came(left, core, 0, h, 0)
        self.put(self.slot(left * 2 + core, 0, h), left, core, 0, h, 4, {"tp_0": right})
        self.came(right, core, h, h, 2)
        self.put(self.slot(right * 2 + core, h, h), right, core, h, h, 5, {"tp_0": left})
        self.came(left, core, h, h, 1)
        self.put(self.slot(left * 2 + core, 0, self.rows), left, core, 0, self.rows, 7, over)
        self.came(right, core, 0, h, 3)
        self.put(self.slot(right * 2 + core, 0, self.rows), right, core, 0, self.rows, 8, over)

    def finish(self):
        core, h, n = self.core, self.half, self.rows
        far, over = self.index(2), {"tp_1": 1 - core}
        self.came(far, core, 0, h, 4)
        self.came(far, core, h, h, 5)
        self.put(self.slot(far * 2 + core, 0, n), far, core, 0, n, 9, over)
        for sem, steps in ((6, 0), (7, -1), (8, 1), (9, 2)):
            self.came(self.index(steps), 1 - core, 0, n, sem)

    def drain(self):
        for copy in self.sent:
            copy.wait_send()


GATHER_SEMS = 10


def first_kernel(
    sizes, part_ref, lat_ref, w_ref, mod_ref, all_ref, wall_ref,
    ybuf, zbuf, tbuf, ysum, zsum, w_yz, w_zy,
    y_send, y_recv, z_send, z_recv, t_send, t_recv, g_send, g_recv,
    wa_send, wa_recv, wb_send, wb_recv, wc_send, wc_recv, wd_send, wd_recv,
):
    ny, nz, nx = sizes
    at = place()
    y, z, x, core = at["sp_1"], at["sp_0"], at["tp_0"], at["tp_1"]
    t = x * 2 + core
    tps = tp_peers(at, nx)
    greet(line_peers(at, "sp_1", ny) + line_peers(at, "sp_0", nz) + tps)
    along_y = Line(at, "sp_1", ny, y_send, y_recv)
    along_z = Line(at, "sp_0", nz, z_send, z_recv)
    along_y.start(lambda there: part_ref, ybuf)
    rows = lat_ref.shape[0]
    gather = Gather(at, nx, rows, lambda s, a, n: all_ref.at[s, pl.ds(a, n)], (g_send, g_recv))
    gather.start(lambda a, n: lat_ref.at[pl.ds(a, n)])
    depth = w_ref.shape[0]
    lanes = pl.ds(pl.multiple_of(t * 256, 256), 128)
    w_yz[z, y] = w_ref[:, lanes]
    lanes = pl.ds(pl.multiple_of(t * 256 + 128, 128), 128)
    w_zy[y, z] = w_ref[:, lanes]
    all_ref[t] = lat_ref[...]
    ybuf[y] = part_ref[...]
    along_y.wait(ybuf)
    ysum[...] = sum(ybuf[k] for k in range(ny))
    along_z.start(lambda there: ysum, zbuf)
    wa = Line(at, "sp_1", ny, wa_send, wa_recv)
    wa.start(lambda there: w_yz.at[z, y], w_yz.at[z])
    wb = Line(at, "sp_0", nz, wb_send, wb_recv)
    wb.start(lambda there: w_zy.at[y, z], w_zy.at[y])
    zbuf[z] = ysum[...]
    gather.forward()
    along_z.wait(zbuf)
    zsum[...] = sum(zbuf[k] for k in range(nz))
    sent = []
    for k, peer in enumerate(tps):
        copy = remote(zsum, tbuf.at[t], t_send.at[k], t_recv.at[t], peer)
        copy.start()
        sent.append(copy)
    tbuf[t] = zsum[...]
    gather.finish()
    wa.wait(w_yz.at[z])
    wc = Line(at, "sp_0", nz, wc_send, wc_recv)
    wc.start(lambda there: w_yz.at[z], w_yz)
    wb.wait(w_zy.at[y])
    wd = Line(at, "sp_1", ny, wd_send, wd_recv)
    wd.start(lambda there: w_zy.at[y], w_zy)
    for k, peer in enumerate(tps):
        s = peer.get("tp_0", x) * 2 + peer["tp_1"]
        remote(tbuf.at[s], tbuf.at[s], t_send.at[k], t_recv.at[s], peer).wait_recv()
    for s in range(2 * nx):
        mod_ref[:, s * 256 : (s + 1) * 256] = tbuf[s]
    wc.wait(w_yz)
    wd.wait(w_zy)
    for a in range(nz):
        for b in range(ny):
            first = (a * ny + b) * depth
            wall_ref[first : first + depth, 0:128] = w_yz[a, b]
            wall_ref[first : first + depth, 128:256] = w_zy[b, a]
    for line in (along_y, along_z, wa, wb, wc, wd, gather):
        line.drain()
    for copy in sent:
        copy.wait_send()


def head_masks(heads):
    lane = lax.broadcasted_iota(jnp.int32, (1, heads * HEAD), 1)
    return [(lane >= h * HEAD) & (lane < (h + 1) * HEAD) for h in range(heads)]


def squeezed(full, masks):
    return sum(
        jnp.where(m, full[h * HEAD : (h + 1) * HEAD], 0.0) for h, m in enumerate(masks)
    )


def spread_out(packed, masks):
    return jnp.concatenate([jnp.where(m, packed, 0.0) for m in masks], axis=0)


def rotated(u, cos, sin, low):
    width = u.shape[1]
    partner = jnp.where(low, pltpu.roll(u, width - HALF, 1), pltpu.roll(u, HALF, 1))
    return u * cos + partner * sin


def outer(keys, values):
    return lax.dot_general(
        keys.astype(BF16), values, (((0,), (0,)), ((), ())), preferred_element_type=F32
    )


def project_kernel(
    sizes, ctx_len, all_ref, ctx_ref, mod_ref, gain_ref, wq_ref, wk_ref, wv_ref,
    cos_ref, sin_ref, base_ref, ld_ref,
    q_ref, k_ref, v_ref, u_ref, st_ref, normed,
):
    ny, nz, nx = sizes
    tokens, width = q_ref.shape
    heads = width // HEAD
    ctx_rows = ctx_ref.shape[0]
    gain = gain_ref[...]

    def norm(rows, c):
        wide = rows.astype(F32)
        r = lax.rsqrt(jnp.mean(wide * wide, axis=-1, keepdims=True) + EPSILON)
        scale = gain * (1.0 + mod_ref[3 * c + 1 : 3 * c + 2])
        return (wide * r * scale + mod_ref[3 * c : 3 * c + 1]).astype(BF16)

    @pl.loop(0, tokens // 64)
    def _(i):
        rows = pl.ds(pl.multiple_of(i * 64, 64), 64)
        normed[rows] = norm(all_ref[rows], 0)

    normed[tokens : tokens + ctx_rows] = norm(ctx_ref[...], 1)
    lane = lax.broadcasted_iota(jnp.int32, (1, width), 1)
    low = lax.rem(lane, HEAD) < HALF
    sign = jnp.where(low, -1.0, 1.0)
    cos_off, sin_off = cos_ref[...], sin_ref[...]
    cos = base_ref[0:1] * cos_off - base_ref[1:2] * sin_off
    sin = (base_ref[1:2] * cos_off + base_ref[0:1] * sin_off) * sign
    ccos = base_ref[2:3] * cos_off[:ctx_rows] - base_ref[3:4] * sin_off[:ctx_rows]
    csin = (base_ref[3:4] * cos_off[:ctx_rows] + base_ref[2:3] * sin_off[:ctx_rows]) * sign
    both = normed[...]
    k_all = jnp.dot(both, wk_ref[...], preferred_element_type=F32)
    v_all = jnp.dot(both, wv_ref[...], preferred_element_type=F32).astype(BF16)
    v_ref[...] = v_all[:tokens]
    k_ref[...] = rotated(k_all[:tokens], cos, sin, low).astype(BF16)
    ck = rotated(k_all[tokens:], ccos, csin, low).astype(BF16).astype(F32)
    cv = v_all[tokens:]
    masks = head_masks(heads)
    ldf, ldb = ld_ref[0:1], ld_ref[1:2]
    sp = lax.axis_index("sp_0") * ny + lax.axis_index("sp_1")
    spot = (sp * ctx_rows + lax.broadcasted_iota(jnp.int32, (ctx_rows, 1), 0)).astype(F32)
    cf = squeezed(outer(ck * jnp.exp(ldf * (ctx_len - 1.0 - spot)), cv), masks)
    cb = squeezed(outer(ck * jnp.exp(ldb * spot), cv), masks)
    at = lax.broadcasted_iota(jnp.int32, (BLOCK, 1), 0).astype(F32)
    to_end, to_start = jnp.exp(ldf * (BLOCK - 1.0 - at)), jnp.exp(ldb * at)
    blocks = tokens // BLOCK
    gf, gb = jnp.exp(ldf * BLOCK), jnp.exp(ldb * BLOCK)
    sf = jnp.zeros((HEAD, width), F32)
    ub = []
    for b in range(blocks):
        keys = k_ref[b * BLOCK : (b + 1) * BLOCK].astype(F32)
        values = v_ref[b * BLOCK : (b + 1) * BLOCK]
        u_ref[b] = sf
        sf = gf * sf + squeezed(outer(keys * to_end, values), masks)
        ub.append(squeezed(outer(keys * to_start, values), masks))
    sb = jnp.zeros((HEAD, width), F32)
    for b in reversed(range(blocks)):
        u_ref[blocks + b] = sb
        sb = gb * sb + ub[b]
    part = HEAD // ny
    for s in range(ny):
        rows = slice(s * part, (s + 1) * part)
        st_ref[s] = jnp.concatenate([sf[rows], sb[rows], cf[rows], cb[rows]], axis=0).astype(BF16)
    q_all = jnp.dot(both[:tokens], wq_ref[...], preferred_element_type=F32)
    q_ref[...] = (rotated(q_all, cos, sin, low) * HEAD ** (-0.5)).astype(BF16)


def state_kernel(
    sizes, tokens, st_ref, ld_ref, ent_ref, r1, s2, r2, s3,
    a_send, a_recv, b_send, b_recv, c_send, c_recv,
):
    ny, nz, nx = sizes
    at = place()
    y, z = at["sp_1"], at["sp_0"]
    greet(line_peers(at, "sp_1", ny) + line_peers(at, "sp_0", nz))
    part = HEAD // ny
    one = Line(at, "sp_1", ny, a_send, a_recv)
    one.start(lambda there: st_ref.at[there], r1)
    ldf, ldb = ld_ref[0:1], ld_ref[1:2]
    r1[y] = st_ref[y]
    one.wait(r1)
    got = [r1[j].astype(F32) for j in range(ny)]
    gf, gb = jnp.exp(ldf * tokens), jnp.exp(ldb * tokens)
    ahead = [jnp.zeros_like(got[0][:part])]
    for j in range(ny):
        ahead.append(gf * ahead[-1] + got[j][:part])
    total_f = ahead.pop()
    behind = [jnp.zeros_like(ahead[0])]
    for j in reversed(range(ny)):
        behind.append(gb * behind[-1] + got[j][part : 2 * part])
    total_b = behind.pop()
    behind = behind[::-1]
    ctx = sum(got)
    ctx_f, ctx_b = ctx[2 * part : 3 * part], ctx[3 * part :]
    row = float(tokens * ny)
    for k in range(nz):
        there = lax.rem(z + k, nz)
        gap = (there - z).astype(F32)
        to_f = jnp.where(there > z, 1.0, 0.0) * jnp.exp(ldf * (row * jnp.maximum(gap - 1.0, 0.0)))
        to_b = jnp.where(there < z, 1.0, 0.0) * jnp.exp(ldb * (row * jnp.maximum(-gap - 1.0, 0.0)))
        start_f = jnp.exp(ldf * (row * there.astype(F32)))
        start_b = jnp.exp(ldb * (row * (nz - 1 - there).astype(F32)))
        s2[there] = jnp.concatenate(
            [to_f * total_f + start_f * ctx_f, to_b * total_b + start_b * ctx_b], axis=0
        ).astype(BF16)
    r2[z] = s2[z]
    two = Line(at, "sp_0", nz, b_send, b_recv)
    two.start(lambda there: s2.at[there], r2)
    two.wait(r2)
    entering = sum(r2[j].astype(F32) for j in range(nz))
    for j in range(ny):
        s3[j] = jnp.concatenate(
            [
                ahead[j] + jnp.exp(ldf * float(tokens * j)) * entering[:part],
                behind[j] + jnp.exp(ldb * float(tokens * (ny - 1 - j))) * entering[part:],
            ],
            axis=0,
        ).astype(BF16)
    three = Line(at, "sp_1", ny, c_send, c_recv)
    three.start(lambda there: s3.at[there], ent_ref)
    ent_ref[y] = s3[y]
    three.wait(ent_ref)
    for line in (one, two, three):
        line.drain()


def averaged(values, average):
    high = values.astype(BF16)
    rest = (values - high.astype(F32)).astype(BF16)
    return jnp.dot(high, average, preferred_element_type=F32) + jnp.dot(
        rest, average, preferred_element_type=F32
    )


def retain_kernel(sizes, q_ref, k_ref, v_ref, u_ref, ent_ref, ld_ref, hg_ref, out_ref, decay):
    ny, nz, nx = sizes
    tokens, width = q_ref.shape
    heads = width // HEAD
    blocks = tokens // BLOCK
    part = HEAD // ny
    masks = head_masks(heads)
    ldf, ldb = ld_ref[0:1], ld_ref[1:2]
    row = lax.broadcasted_iota(jnp.int32, (BLOCK, BLOCK), 0)
    col = lax.broadcasted_iota(jnp.int32, (BLOCK, BLOCK), 1)
    gap = (row - col).astype(F32)
    for h in range(heads):
        f, b = ldf[:, h * HEAD : h * HEAD + 1], ldb[:, h * HEAD : h * HEAD + 1]
        decay[h * BLOCK : (h + 1) * BLOCK] = jnp.where(
            gap >= 0, jnp.exp(f * jnp.maximum(gap, 0.0)), 0.0
        ) + jnp.where(gap <= 0, jnp.exp(b * jnp.maximum(-gap, 0.0)), 0.0)
    ent = [ent_ref[s].astype(F32) for s in range(ny)]
    enter_f = jnp.concatenate([e[:part] for e in ent], axis=0)
    enter_b = jnp.concatenate([e[part:] for e in ent], axis=0)
    at = lax.broadcasted_iota(jnp.int32, (BLOCK, 1), 0).astype(F32)
    read_f, read_b = jnp.exp(ldf * (at + 1.0)), jnp.exp(ldb * (BLOCK - at))
    a = lax.broadcasted_iota(jnp.int32, (width, width), 0)
    b = lax.broadcasted_iota(jnp.int32, (width, width), 1)
    average = jnp.where(a // HEAD == b // HEAD, 1.0 / HEAD, 0.0).astype(BF16)
    for i in range(blocks):
        rows = slice(i * BLOCK, (i + 1) * BLOCK)
        q = q_ref[rows]
        wide = q.astype(F32)
        stacked = jnp.concatenate([jnp.where(m, wide, 0.0) for m in masks], axis=0).astype(BF16)
        scores = lax.dot_general(
            stacked, k_ref[rows], (((1,), (1,)), ((), ())), preferred_element_type=F32
        )
        weights = (scores * decay[...]).astype(BF16)
        inside = jnp.dot(weights, v_ref[rows], preferred_element_type=F32)
        state_f = u_ref[i] + jnp.exp(ldf * float(BLOCK * i)) * enter_f
        state_b = u_ref[blocks + i] + jnp.exp(ldb * float(BLOCK * (blocks - 1 - i))) * enter_b
        states = jnp.concatenate(
            [spread_out(state_f, masks), spread_out(state_b, masks)], axis=0
        ).astype(BF16)
        readers = jnp.concatenate([wide * read_f, wide * read_b], axis=1).astype(BF16)
        o = jnp.dot(readers, states, preferred_element_type=F32)
        for h, m in enumerate(masks):
            o = o + jnp.where(m, inside[h * BLOCK : (h + 1) * BLOCK], 0.0)
        centred = o - averaged(o, average)
        spread = averaged(centred * centred, average)
        out_ref[rows] = (centred * lax.rsqrt(spread + EPSILON) * hg_ref[...]).astype(BF16)


def output_kernel(
    sizes, ret_ref, wall_ref, all_ref, mod_ref, out_ref, gathered, done, landed,
    g_send, g_recv, o_send, o_recv,
):
    ny, nz, nx = sizes
    at = place()
    x, core = at["tp_0"], at["tp_1"]
    t = x * 2 + core
    tps = tp_peers(at, nx)
    greet(tps)
    tokens, width = ret_ref.shape
    own_rows = out_ref.shape[0]
    chunk = 2 * own_rows
    chunks = tokens // chunk
    gathers = []
    for c in range(chunks):
        g = Gather(
            at, nx, chunk, lambda s, a, n, c=c: gathered.at[s, pl.ds(c * chunk + a, n)],
            (g_send.at[c], g_recv.at[c]),
        )
        g.start(lambda a, n, c=c: ret_ref.at[pl.ds(c * chunk + a, n)])
        gathers.append(g)
    gathered[t] = ret_ref[...]
    gate_row = mod_ref[2:3, pl.ds(pl.multiple_of(t * width, width), width)]
    sent = []
    for g in gathers:
        g.forward()
    for c, g in enumerate(gathers):
        g.finish()
        rows = slice(c * chunk, (c + 1) * chunk)
        mixed = sum(
            jnp.dot(
                gathered[s, rows], wall_ref[s * width : (s + 1) * width],
                preferred_element_type=F32,
            )
            for s in range(2 * nx)
        )
        lat = all_ref[rows, pl.ds(pl.multiple_of(t * width, width), width)].astype(F32)
        result = (lat + gate_row * mixed).astype(BF16)
        done[2 * c] = result[:own_rows]
        done[2 * c + 1] = result[own_rows:]
        for k in range(2):
            owner = 2 * c + k
            copy = remote(
                done.at[owner], landed.at[t], o_send.at[owner], o_recv.at[t],
                {"tp_0": jnp.int32(c), "tp_1": jnp.int32(k)},
            )
            mine = owner == t

            @pl.when(jnp.logical_not(mine))
            def _(copy=copy):
                copy.start()

            sent.append((mine, copy))
    landed[t] = done[t]
    for k, peer in enumerate(tps):
        s = peer.get("tp_0", x) * 2 + peer["tp_1"]
        remote(landed.at[s], landed.at[s], o_send.at[0], o_recv.at[s], peer).wait_recv()
    for s in range(2 * nx):
        out_ref[:, s * width : (s + 1) * width] = landed[s]
    for g in gathers:
        g.drain()
    for mine, copy in sent:

        @pl.when(jnp.logical_not(mine))
        def _(copy=copy):
            copy.wait_send()


def call(kernel, outs, scratch, collective, ins):
    spec = pl.BlockSpec(memory_space=pltpu.VMEM)
    more = {} if collective is None else {"collective_id": collective, "has_side_effects": True}
    return pl.pallas_call(
        kernel,
        out_shape=outs,
        in_specs=[spec] * len(ins),
        out_specs=jax.tree.map(lambda _: spec, outs),
        scratch_shapes=scratch,
        compiler_params=pltpu.CompilerParams(vmem_limit_bytes=VMEM_LIMIT, **more),
    )(*ins)


def turns(positions):
    frequency = ROTARY_BASE ** -np.linspace(0.0, 1.0, HALF)
    angles = np.asarray(positions, np.float64)[:, None] * frequency[None]
    return np.cos(angles), np.sin(angles)


def per_device(
    sizes, latent, context, condition, context_condition, modulation_weight, norm_gain,
    query_weight, key_weight, value_weight, log_decay, head_gain, output_weight,
):
    ny, nz, nx = sizes
    nt = 2 * nx
    d = latent.shape[1]
    width = query_weight.shape[1]
    heads = width // HEAD
    own = latent.shape[0]
    tokens = own * nt
    ctx_rows = context.shape[0]
    ctx_len = ctx_rows * ny * nz
    seq = lax.axis_index(SP)
    dma = pltpu.SemaphoreType.DMA
    activated = jax.nn.silu(jnp.stack([condition, context_condition])).astype(BF16)
    depth, _, cols = modulation_weight.shape
    mine = lax.dynamic_slice_in_dim(activated, seq * depth, depth, 1)
    part = jnp.dot(
        mine, modulation_weight.reshape(depth, 3 * cols), preferred_element_type=F32
    ).reshape(6, cols)
    part = jnp.pad(part, ((0, 2), (0, 0)))
    wrows = output_weight.shape[0]
    modulation, rows, wall = call(
        functools.partial(first_kernel, sizes),
        [
            jax.ShapeDtypeStruct((8, d), F32),
            jax.ShapeDtypeStruct((nt, own, d), BF16),
            jax.ShapeDtypeStruct((output_weight.shape[0] * ny * nz, cols), BF16),
        ],
        [
            pltpu.VMEM((ny, 8, cols), F32), pltpu.VMEM((nz, 8, cols), F32),
            pltpu.VMEM((nt, 8, cols), F32), pltpu.VMEM((8, cols), F32), pltpu.VMEM((8, cols), F32),
            pltpu.VMEM((nz, ny, wrows, 128), BF16), pltpu.VMEM((ny, nz, wrows, 128), BF16),
            dma((ny,)), dma((ny,)), dma((nz,)), dma((nz,)), dma((nt,)), dma((nt,)),
            dma((GATHER_SEMS,)), dma((GATHER_SEMS,)),
            dma((ny,)), dma((ny,)), dma((nz,)), dma((nz,)),
            dma((nz,)), dma((nz,)), dma((ny,)), dma((ny,)),
        ],
        0,
        [part, latent, output_weight],
    )
    rows = rows.reshape(tokens, d)
    tile = lambda a: np.tile(np.asarray(a, np.float32), (1, heads * 2))
    cos_off, sin_off = (jnp.asarray(tile(a)) for a in turns(np.arange(tokens)))
    bases = np.stack(
        [tile(a) for a in turns(ctx_len + tokens * np.arange(ny * nz))]
        + [tile(a) for a in turns(ctx_rows * np.arange(ny * nz))],
        axis=1,
    )
    base = lax.dynamic_index_in_dim(jnp.asarray(bases), seq, 0, keepdims=False)
    rates = jnp.repeat(log_decay, HEAD, axis=1)
    blocks = tokens // BLOCK
    part_rows = HEAD // ny
    q, k, v, u, st = call(
        functools.partial(project_kernel, sizes, ctx_len),
        [
            jax.ShapeDtypeStruct((tokens, width), BF16),
            jax.ShapeDtypeStruct((tokens, width), BF16),
            jax.ShapeDtypeStruct((tokens, width), BF16),
            jax.ShapeDtypeStruct((2 * blocks, HEAD, width), F32),
            jax.ShapeDtypeStruct((ny, 4 * part_rows, width), BF16),
        ],
        [pltpu.VMEM((tokens + ctx_rows, d), BF16)],
        None,
        [
            rows, context, modulation, norm_gain.reshape(1, d), query_weight, key_weight,
            value_weight, cos_off, sin_off, base, rates,
        ],
    )
    entering = call(
        functools.partial(state_kernel, sizes, tokens),
        jax.ShapeDtypeStruct((ny, 2 * part_rows, width), BF16),
        [
            pltpu.VMEM((ny, 4 * part_rows, width), BF16),
            pltpu.VMEM((nz, 2 * part_rows, width), BF16),
            pltpu.VMEM((nz, 2 * part_rows, width), BF16),
            pltpu.VMEM((ny, 2 * part_rows, width), BF16),
            dma((ny,)), dma((ny,)), dma((nz,)), dma((nz,)), dma((ny,)), dma((ny,)),
        ],
        1,
        [st, rates],
    )
    retained = call(
        functools.partial(retain_kernel, sizes),
        jax.ShapeDtypeStruct((tokens, width), BF16),
        [pltpu.VMEM((heads * BLOCK, BLOCK), F32)],
        None,
        [q, k, v, u, entering, rates, head_gain.reshape(1, width)],
    )
    chunks = tokens // (2 * own)
    return call(
        functools.partial(output_kernel, sizes),
        jax.ShapeDtypeStruct((own, d), BF16),
        [
            pltpu.VMEM((nt, tokens, width), BF16),
            pltpu.VMEM((nt, own, width), BF16),
            pltpu.VMEM((nt, own, width), BF16),
            dma((chunks, GATHER_SEMS)), dma((chunks, GATHER_SEMS)), dma((nt,)), dma((nt,)),
        ],
        2,
        [retained, wall, rows, modulation],
    )


def solution(mesh, ny=8, nz=8, nx=4):
    split = Mesh(mesh.devices.reshape(nz, ny, nx, 2), SP_TP)
    placed = (
        P(SP_TP, None), P(SP, None), P(), P(), P(SP, None, TP), P(), P(None, TP), P(None, TP),
        P(None, TP), P(None, TP), P(TP), P(SP, None),
    )
    return jax.shard_map(
        functools.partial(per_device, (ny, nz, nx)), mesh=split, in_specs=placed,
        out_specs=P(SP_TP, None), check_vma=False,
    )
```

```python
import functools

import jax
import jax.numpy as jnp
import numpy as np
from jax import lax
from jax.experimental import pallas as pl
from jax.experimental.pallas import tpu as pltpu
from jax.sharding import Mesh
from jax.sharding import PartitionSpec as P

HEAD = 64
HALF = HEAD // 2
BLOCK = 128
SP = ("sp_0", "sp_1")
TP = ("tp_0", "tp_1")
SP_TP = SP + TP
EPSILON = 1e-06
ROTARY_BASE = 10000.0
F32, BF16 = jnp.float32, jnp.bfloat16
MESH = pl.DeviceIdType.MESH
VMEM_LIMIT = 60 * 1024 * 1024


def remote(src, dst, send_sem, recv_sem, device):
    return pltpu.make_async_remote_copy(
        src_ref=src, dst_ref=dst, send_sem=send_sem, recv_sem=recv_sem,
        device_id=device, device_id_type=MESH,
    )


def place():
    return {a: lax.axis_index(a) for a in SP_TP}


def tp_peers(at, nx):
    core, x = at["tp_1"], at["tp_0"]
    peers = [{"tp_0": x, "tp_1": 1 - core}]
    for k in range(1, nx):
        there = lax.rem(x + k, nx)
        peers += [{"tp_0": there, "tp_1": core}, {"tp_0": there, "tp_1": 1 - core}]
    return peers


def line_peers(at, axis, n):
    return [{axis: lax.rem(at[axis] + k, n)} for k in range(1, n)]


def greet(peers):
    barrier = pltpu.get_barrier_semaphore()
    for peer in peers:
        pl.semaphore_signal(barrier, inc=1, device_id=peer, device_id_type=MESH)
    return lambda: pl.semaphore_wait(barrier, len(peers))


class Line:
    def __init__(self, at, axis, n, send_sems, recv_sems):
        self.me, self.axis, self.n = at[axis], axis, n
        self.send_sems, self.recv_sems = send_sems, recv_sems
        self.sent = []

    def start(self, source_of, slots):
        for k in range(1, self.n):
            there = lax.rem(self.me + k, self.n)
            copy = remote(
                source_of(there), slots.at[self.me], self.send_sems.at[k],
                self.recv_sems.at[self.me], {self.axis: there},
            )
            copy.start()
            self.sent.append(copy)

    def wait(self, slots):
        for k in range(1, self.n):
            source = lax.rem(self.me + self.n - k, self.n)
            remote(
                slots.at[source], slots.at[source], self.send_sems.at[k],
                self.recv_sems.at[source], {self.axis: source},
            ).wait_recv()

    def drain(self):
        for copy in self.sent:
            copy.wait_send()


class Gather:
    def __init__(self, at, nx, rows, slot, sems):
        self.x, self.core, self.nx, self.rows, self.slot = at["tp_0"], at["tp_1"], nx, rows, slot
        self.send_sems, self.recv_sems = sems
        self.half = rows // 2
        self.sent = []

    def index(self, steps):
        return lax.rem(self.x + self.nx + steps, self.nx)

    def put(self, src, x_of, core_of, first, count, sem, device):
        copy = remote(
            src, self.slot(x_of * 2 + core_of, first, count), self.send_sems.at[sem],
            self.recv_sems.at[sem], device,
        )
        copy.start()
        self.sent.append(copy)

    def came(self, x_of, core_of, first, count, sem):
        view = self.slot(x_of * 2 + core_of, first, count)
        remote(view, view, self.send_sems.at[sem], self.recv_sems.at[sem], {"tp_0": self.x}).wait_recv()

    def start(self, own):
        x, core, h = self.x, self.core, self.half
        right, left = {"tp_0": self.index(1)}, {"tp_0": self.index(-1)}
        self.put(own(0, h), x, core, 0, h, 0, right)
        self.put(own(h, h), x, core, h, h, 2, left)
        self.put(own(h, h), x, core, h, h, 1, right)
        self.put(own(0, h), x, core, 0, h, 3, left)
        self.put(own(0, self.rows), x, core, 0, self.rows, 6, {"tp_1": 1 - core})

    def forward(self):
        core, h = self.core, self.half
        left, right, over = self.index(-1), self.index(1), {"tp_1": 1 - core}
        self.came(left, core, 0, h, 0)
        self.put(self.slot(left * 2 + core, 0, h), left, core, 0, h, 4, {"tp_0": right})
        self.came(right, core, h, h, 2)
        self.put(self.slot(right * 2 + core, h, h), right, core, h, h, 5, {"tp_0": left})
        self.came(left, core, h, h, 1)
        self.put(self.slot(left * 2 + core, 0, self.rows), left, core, 0, self.rows, 7, over)
        self.came(right, core, 0, h, 3)
        self.put(self.slot(right * 2 + core, 0, self.rows), right, core, 0, self.rows, 8, over)

    def finish(self):
        core, h, n = self.core, self.half, self.rows
        far, over = self.index(2), {"tp_1": 1 - core}
        self.came(far, core, 0, h, 4)
        self.came(far, core, h, h, 5)
        self.put(self.slot(far * 2 + core, 0, n), far, core, 0, n, 9, over)
        for sem, steps in ((6, 0), (7, -1), (8, 1), (9, 2)):
            self.came(self.index(steps), 1 - core, 0, n, sem)

    def drain(self):
        for copy in self.sent:
            copy.wait_send()


GATHER_SEMS = 10


def head_masks(heads):
    lane = lax.broadcasted_iota(jnp.int32, (1, heads * HEAD), 1)
    return [(lane >= h * HEAD) & (lane < (h + 1) * HEAD) for h in range(heads)]


def squeezed(full, masks):
    return sum(
        jnp.where(m, full[h * HEAD : (h + 1) * HEAD], 0.0) for h, m in enumerate(masks)
    )


def spread_out(packed, masks):
    return jnp.concatenate([jnp.where(m, packed, 0.0) for m in masks], axis=0)


def rotated(u, cos, sin, low):
    width = u.shape[1]
    partner = jnp.where(low, pltpu.roll(u, width - HALF, 1), pltpu.roll(u, HALF, 1))
    return u * cos + partner * sin


def outer(keys, values):
    return lax.dot_general(
        keys.astype(BF16), values, (((0,), (0,)), ((), ())), preferred_element_type=F32
    )


def averaged(values, average):
    high = values.astype(BF16)
    rest = (values - high.astype(F32)).astype(BF16)
    return jnp.dot(high, average, preferred_element_type=F32) + jnp.dot(
        rest, average, preferred_element_type=F32
    )


def whole_kernel(
    sizes, ctx_len, cond_ref, mw_ref, lat_ref, ctx_ref, w_ref, gain_ref, ld_ref, hg_ref,
    cos_ref, sin_ref, base_ref, wq_hbm, wk_hbm, wv_hbm, out_ref,
    wq, wk, wv, part_s, mod, rows_all, stat, normed, cos_s, sin_s, decay,
    ybuf, zbuf, tbuf, ysum, zsum, w_yz, w_zy, wall,
    k_s, v_s, u_s, o_s, readers, st, r1, s2, r2, s3, ent, ret, gathered, done, landed,
    wt_sem, y_send, y_recv, z_send, z_recv, t_send, t_recv, l_send, l_recv,
    wa_send, wa_recv, wb_send, wb_recv, wc_send, wc_recv, wd_send, wd_recv,
    a_send, a_recv, b_send, b_recv, c_send, c_recv, g_send, g_recv, o_send, o_recv,
):
    ny, nz, nx = sizes
    nt = 2 * nx
    own, d = lat_ref.shape
    tokens = own * nt
    width = hg_ref.shape[1]
    heads = width // HEAD
    blocks = tokens // BLOCK
    part = HEAD // ny
    ctx_rows = ctx_ref.shape[0]
    at = place()
    y, z, x, core = at["sp_1"], at["sp_0"], at["tp_0"], at["tp_1"]
    t, sp = x * 2 + core, z * ny + y
    tps = tp_peers(at, nx)
    weights = [
        pltpu.make_async_copy(a, b, wt_sem.at[i])
        for i, (a, b) in enumerate(((wk_hbm, wk), (wv_hbm, wv), (wq_hbm, wq)))
    ]
    for copy in weights:
        copy.start()
    met = greet(line_peers(at, "sp_1", ny) + line_peers(at, "sp_0", nz) + tps)

    c = cond_ref[...]
    activated = (c / (1.0 + jnp.exp(-c))).astype(BF16)
    depth, _, cols = mw_ref.shape
    entry = lax.broadcasted_iota(jnp.int32, (d, depth), 0)
    place_of = lax.broadcasted_iota(jnp.int32, (d, depth), 1) + sp * depth
    mine = jnp.dot(
        activated, jnp.where(entry == place_of, 1.0, 0.0).astype(BF16), preferred_element_type=F32
    ).astype(BF16)
    parts = [jnp.dot(mine, mw_ref[:, r, :], preferred_element_type=F32) for r in range(3)]
    part_s[...] = jnp.concatenate(
        [parts[r][k : k + 1] for k in range(2) for r in range(3)] + [parts[0][2:4]], axis=0
    )
    met()
    along_y = Line(at, "sp_1", ny, y_send, y_recv)
    along_z = Line(at, "sp_0", nz, z_send, z_recv)
    along_y.start(lambda there: part_s, ybuf)
    spread_rows = Gather(
        at, nx, own, lambda s, a, n: rows_all.at[pl.ds(s * own + a, n)], (l_send, l_recv)
    )
    spread_rows.start(lambda a, n: lat_ref.at[pl.ds(a, n)])
    ybuf[y] = part_s[...]
    rows_all[pl.ds(pl.multiple_of(t * own, own), own)] = lat_ref[...]
    wrows = w_ref.shape[0]
    w_yz[z, y] = w_ref[:, pl.ds(pl.multiple_of(t * 256, 256), 128)]
    w_zy[y, z] = w_ref[:, pl.ds(pl.multiple_of(t * 256 + 128, 128), 128)]
    wa = Line(at, "sp_1", ny, wa_send, wa_recv)
    wa.start(lambda there: w_yz.at[z, y], w_yz.at[z])

    lane = lax.broadcasted_iota(jnp.int32, (1, width), 1)
    low = lax.rem(lane, HEAD) < HALF
    sign = jnp.where(low, -1.0, 1.0)
    repeat = lambda a: jnp.concatenate([a] * (width // a.shape[1]), axis=1)
    base = repeat(base_ref[sp])
    cos_off, sin_off = repeat(cos_ref[...]), repeat(sin_ref[...])
    cos_s[...] = base[0:1] * cos_off - base[1:2] * sin_off
    sin_s[...] = (base[1:2] * cos_off + base[0:1] * sin_off) * sign
    ccos = base[2:3] * cos_off[:ctx_rows] - base[3:4] * sin_off[:ctx_rows]
    csin = (base[3:4] * cos_off[:ctx_rows] + base[2:3] * sin_off[:ctx_rows]) * sign
    masks = head_masks(heads)
    rates = sum(jnp.where(m, ld_ref[:, h : h + 1], 0.0) for h, m in enumerate(masks))
    ldf, ldb = rates[0:1], rates[1:2]
    row = lax.broadcasted_iota(jnp.int32, (BLOCK, BLOCK), 0)
    col = lax.broadcasted_iota(jnp.int32, (BLOCK, BLOCK), 1)
    gap = (row - col).astype(F32)
    for h in range(heads):
        f, b = ldf[:, h * HEAD : h * HEAD + 1], ldb[:, h * HEAD : h * HEAD + 1]
        decay[h * BLOCK : (h + 1) * BLOCK] = jnp.where(
            gap >= 0, jnp.exp(f * jnp.maximum(gap, 0.0)), 0.0
        ) + jnp.where(gap <= 0, jnp.exp(b * jnp.maximum(-gap, 0.0)), 0.0)

    along_y.wait(ybuf)
    ysum[...] = sum(ybuf[k] for k in range(ny))
    along_z.start(lambda there: ysum, zbuf)
    zbuf[z] = ysum[...]
    wb = Line(at, "sp_0", nz, wb_send, wb_recv)
    wb.start(lambda there: w_zy.at[y, z], w_zy.at[y])
    spread_rows.forward()
    along_z.wait(zbuf)
    zsum[...] = sum(zbuf[k] for k in range(nz))
    sent = []
    for k, peer in enumerate(tps):
        copy = remote(zsum, tbuf.at[t], t_send.at[k], t_recv.at[t], peer)
        copy.start()
        sent.append(copy)
    tbuf[t] = zsum[...]
    wa.wait(w_yz.at[z])
    wc = Line(at, "sp_0", nz, wc_send, wc_recv)
    wc.start(lambda there: w_yz.at[z], w_yz)
    wb.wait(w_zy.at[y])
    wd = Line(at, "sp_1", ny, wd_send, wd_recv)
    wd.start(lambda there: w_zy.at[y], w_zy)
    spread_rows.finish()

    def root(rows):
        wide = rows.astype(F32)
        return lax.rsqrt(jnp.mean(wide * wide, axis=-1, keepdims=True) + EPSILON)

    @pl.loop(0, tokens // 64)
    def _(i):
        rows = pl.ds(pl.multiple_of(i * 64, 64), 64)
        stat[rows] = jnp.broadcast_to(root(rows_all[rows]), (64, 128))

    ctx_root = root(ctx_ref[...])
    for k, peer in enumerate(tps):
        s = peer.get("tp_0", x) * 2 + peer["tp_1"]
        remote(tbuf.at[s], tbuf.at[s], t_send.at[k], t_recv.at[s], peer).wait_recv()
    for s in range(nt):
        mod[:, s * 256 : (s + 1) * 256] = tbuf[s]

    def norm(rows, r, k):
        scale = gain_ref[...] * (1.0 + mod[3 * k + 1 : 3 * k + 2])
        return (rows.astype(F32) * r * scale + mod[3 * k : 3 * k + 1]).astype(BF16)

    @pl.loop(0, tokens // 64)
    def _(i):
        rows = pl.ds(pl.multiple_of(i * 64, 64), 64)
        normed[rows] = norm(rows_all[rows], stat[rows][:, 0:1], 0)

    normed[tokens : tokens + ctx_rows] = norm(ctx_ref[...], ctx_root, 1)
    weights[0].wait()
    k_all = jnp.dot(normed[...], wk[...], preferred_element_type=F32)
    weights[1].wait()
    v_all = jnp.dot(normed[...], wv[...], preferred_element_type=F32).astype(BF16)
    v_s[...] = v_all[:tokens]
    k_s[...] = rotated(k_all[:tokens], cos_s[...], sin_s[...], low).astype(BF16)
    ck = rotated(k_all[tokens:], ccos, csin, low).astype(BF16).astype(F32)
    cv = v_all[tokens:]
    spot = (sp * ctx_rows + lax.broadcasted_iota(jnp.int32, (ctx_rows, 1), 0)).astype(F32)
    cf = squeezed(outer(ck * jnp.exp(ldf * (ctx_len - 1.0 - spot)), cv), masks)
    cb = squeezed(outer(ck * jnp.exp(ldb * spot), cv), masks)
    l = lax.broadcasted_iota(jnp.int32, (BLOCK, 1), 0).astype(F32)
    to_end, to_start = jnp.exp(ldf * (BLOCK - 1.0 - l)), jnp.exp(ldb * l)
    gf, gb = jnp.exp(ldf * BLOCK), jnp.exp(ldb * BLOCK)
    sf = jnp.zeros((HEAD, width), F32)
    ub = []
    for b in range(blocks):
        keys = k_s[b * BLOCK : (b + 1) * BLOCK].astype(F32)
        values = v_s[b * BLOCK : (b + 1) * BLOCK]
        u_s[b] = sf
        sf = gf * sf + squeezed(outer(keys * to_end, values), masks)
        ub.append(squeezed(outer(keys * to_start, values), masks))
    sb = jnp.zeros((HEAD, width), F32)
    for b in reversed(range(blocks)):
        u_s[blocks + b] = sb
        sb = gb * sb + ub[b]
    for s in range(ny):
        rows = slice(s * part, (s + 1) * part)
        st[s] = jnp.concatenate([sf[rows], sb[rows], cf[rows], cb[rows]], axis=0).astype(BF16)
    one = Line(at, "sp_1", ny, a_send, a_recv)
    one.start(lambda there: st.at[there], r1)
    r1[y] = st[y]

    weights[2].wait()
    q_all = jnp.dot(normed[0:tokens], wq[...], preferred_element_type=F32)
    queries = (rotated(q_all, cos_s[...], sin_s[...], low) * HEAD ** (-0.5)).astype(BF16)
    read_f, read_b = jnp.exp(ldf * (l + 1.0)), jnp.exp(ldb * (BLOCK - l))
    for i in range(blocks):
        rows = slice(i * BLOCK, (i + 1) * BLOCK)
        wide = queries[rows].astype(F32)
        stacked = jnp.concatenate([jnp.where(m, wide, 0.0) for m in masks], axis=0).astype(BF16)
        scores = lax.dot_general(
            stacked, k_s[rows], (((1,), (1,)), ((), ())), preferred_element_type=F32
        )
        inside = jnp.dot(
            (scores * decay[...]).astype(BF16), v_s[rows], preferred_element_type=F32
        )
        states = jnp.concatenate(
            [spread_out(u_s[i], masks), spread_out(u_s[blocks + i], masks)], axis=0
        ).astype(BF16)
        near_f, near_b = wide * read_f, wide * read_b
        o = jnp.dot(
            jnp.concatenate([near_f, near_b], axis=1).astype(BF16), states,
            preferred_element_type=F32,
        )
        for h, m in enumerate(masks):
            o = o + jnp.where(m, inside[h * BLOCK : (h + 1) * BLOCK], 0.0)
        o_s[rows] = o
        far_f = wide * jnp.exp(ldf * (l + (i * BLOCK + 1.0)))
        far_b = wide * jnp.exp(ldb * ((tokens - i * BLOCK) - l))
        readers[rows] = jnp.concatenate([far_f, far_b], axis=1).astype(BF16)

    one.wait(r1)
    got = [r1[j].astype(F32) for j in range(ny)]
    hf, hb = jnp.exp(ldf * tokens), jnp.exp(ldb * tokens)
    ahead = [jnp.zeros_like(got[0][:part])]
    for j in range(ny):
        ahead.append(hf * ahead[-1] + got[j][:part])
    total_f = ahead.pop()
    behind = [jnp.zeros_like(ahead[0])]
    for j in reversed(range(ny)):
        behind.append(hb * behind[-1] + got[j][part : 2 * part])
    total_b = behind.pop()
    behind = behind[::-1]
    ctx = sum(got)
    ctx_f, ctx_b = ctx[2 * part : 3 * part], ctx[3 * part :]
    span = float(tokens * ny)
    for k in range(nz):
        there = lax.rem(z + k, nz)
        ahead_by = (there - z).astype(F32)
        to_f = jnp.where(there > z, 1.0, 0.0) * jnp.exp(ldf * (span * jnp.maximum(ahead_by - 1.0, 0.0)))
        to_b = jnp.where(there < z, 1.0, 0.0) * jnp.exp(ldb * (span * jnp.maximum(-ahead_by - 1.0, 0.0)))
        start_f = jnp.exp(ldf * (span * there.astype(F32)))
        start_b = jnp.exp(ldb * (span * (nz - 1 - there).astype(F32)))
        s2[there] = jnp.concatenate(
            [to_f * total_f + start_f * ctx_f, to_b * total_b + start_b * ctx_b], axis=0
        ).astype(BF16)
    two = Line(at, "sp_0", nz, b_send, b_recv)
    two.start(lambda there: s2.at[there], r2)
    r2[z] = s2[z]
    wc.wait(w_yz)
    two.wait(r2)
    entering = sum(r2[j].astype(F32) for j in range(nz))
    for j in range(ny):
        s3[j] = jnp.concatenate(
            [
                ahead[j] + jnp.exp(ldf * float(tokens * j)) * entering[:part],
                behind[j] + jnp.exp(ldb * float(tokens * (ny - 1 - j))) * entering[part:],
            ],
            axis=0,
        ).astype(BF16)
    three = Line(at, "sp_1", ny, c_send, c_recv)
    three.start(lambda there: s3.at[there], ent)
    ent[y] = s3[y]
    wd.wait(w_zy)
    for a in range(nz):
        for b in range(ny):
            first = (a * ny + b) * wrows
            wall[first : first + wrows, 0:128] = w_yz[a, b]
            wall[first : first + wrows, 128:256] = w_zy[b, a]
    a = lax.broadcasted_iota(jnp.int32, (width, width), 0)
    b = lax.broadcasted_iota(jnp.int32, (width, width), 1)
    average = jnp.where(a // HEAD == b // HEAD, 1.0 / HEAD, 0.0).astype(BF16)
    three.wait(ent)

    slices = [ent[s].astype(F32) for s in range(ny)]
    states = jnp.concatenate(
        [
            spread_out(jnp.concatenate([e[:part] for e in slices], axis=0), masks),
            spread_out(jnp.concatenate([e[part:] for e in slices], axis=0), masks),
        ],
        axis=0,
    ).astype(BF16)
    chunk = 2 * own
    gathers = []
    for c in range(nx):
        rows = slice(c * chunk, (c + 1) * chunk)
        o = o_s[rows] + jnp.dot(readers[rows], states, preferred_element_type=F32)
        centred = o - averaged(o, average)
        spread = averaged(centred * centred, average)
        ret[rows] = (centred * lax.rsqrt(spread + EPSILON) * hg_ref[...]).astype(BF16)
        g = Gather(
            at, nx, chunk, lambda s, a, n, c=c: gathered.at[s, pl.ds(c * chunk + a, n)],
            (g_send.at[c], g_recv.at[c]),
        )
        g.start(lambda a, n, c=c: ret.at[pl.ds(c * chunk + a, n)])
        gathers.append(g)
        gathered[t, rows] = ret[rows]
    columns = pl.ds(pl.multiple_of(t * width, width), width)
    gate_row = mod[2:3, columns]
    for g in gathers:
        g.forward()
    posted = []
    for c, g in enumerate(gathers):
        g.finish()
        rows = slice(c * chunk, (c + 1) * chunk)
        mixed = sum(
            jnp.dot(
                gathered[s, rows], wall[s * width : (s + 1) * width], preferred_element_type=F32
            )
            for s in range(nt)
        )
        result = (rows_all[rows, columns].astype(F32) + gate_row * mixed).astype(BF16)
        done[2 * c] = result[:own]
        done[2 * c + 1] = result[own:]
        for k in range(2):
            owner = 2 * c + k
            copy = remote(
                done.at[owner], landed.at[t], o_send.at[owner], o_recv.at[t],
                {"tp_0": jnp.int32(c), "tp_1": jnp.int32(k)},
            )
            other = jnp.logical_not(owner == t)

            @pl.when(other)
            def _(copy=copy):
                copy.start()

            posted.append((other, copy))
    landed[t] = done[t]
    for k, peer in enumerate(tps):
        s = peer.get("tp_0", x) * 2 + peer["tp_1"]
        remote(landed.at[s], landed.at[s], o_send.at[0], o_recv.at[s], peer).wait_recv()
    for s in range(nt):
        out_ref[:, s * width : (s + 1) * width] = landed[s]
    for line in (along_y, along_z, wa, wb, wc, wd, one, two, three, spread_rows, *gathers):
        line.drain()
    for copy in sent:
        copy.wait_send()
    for other, copy in posted:

        @pl.when(other)
        def _(copy=copy):
            copy.wait_send()


def turns(positions):
    frequency = ROTARY_BASE ** -np.linspace(0.0, 1.0, HALF)
    angles = np.asarray(positions, np.float64)[:, None] * frequency[None]
    tile = lambda a: np.tile(np.asarray(a, np.float32), (1, 128 // HALF))
    return tile(np.cos(angles)), tile(np.sin(angles))


def per_device(
    sizes, latent, context, condition, context_condition, modulation_weight, norm_gain,
    query_weight, key_weight, value_weight, log_decay, head_gain, output_weight,
):
    ny, nz, nx = sizes
    nt = 2 * nx
    d = latent.shape[1]
    width = query_weight.shape[1]
    heads = width // HEAD
    own = latent.shape[0]
    tokens = own * nt
    ctx_rows = context.shape[0]
    ctx_len = ctx_rows * ny * nz
    wrows = output_weight.shape[0]
    cos_off, sin_off = turns(np.arange(tokens))
    bases = np.stack(
        turns(ctx_len + tokens * np.arange(ny * nz)) + turns(ctx_rows * np.arange(ny * nz)), axis=1
    )
    cond = jnp.concatenate(
        [condition[None], context_condition[None], jnp.zeros((6, d), F32)], axis=0
    )
    ins = [
        cond, modulation_weight, latent, context, output_weight, norm_gain.reshape(1, d),
        log_decay, head_gain.reshape(1, width), jnp.asarray(cos_off), jnp.asarray(sin_off),
        jnp.asarray(bases), query_weight, key_weight, value_weight,
    ]
    dma = lambda *n: pltpu.SemaphoreType.DMA(n)
    part, blocks = HEAD // ny, tokens // BLOCK
    pair = lambda n: [dma(n), dma(n)]
    scratch = [
        pltpu.VMEM(shape, kind)
        for shape, kind in (
            *[((d, width), BF16)] * 3,
            ((8, width), F32), ((8, d), F32), ((tokens, d), BF16), ((tokens, 128), F32),
            ((tokens + ctx_rows, d), BF16), ((tokens, width), F32), ((tokens, width), F32),
            ((heads * BLOCK, BLOCK), F32),
            ((ny, 8, width), F32), ((nz, 8, width), F32), ((nt, 8, width), F32),
            ((8, width), F32), ((8, width), F32),
            ((nz, ny, wrows, 128), BF16), ((ny, nz, wrows, 128), BF16), ((d, width), BF16),
            ((tokens, width), BF16), ((tokens, width), BF16), ((2 * blocks, HEAD, width), F32),
            ((tokens, width), F32), ((tokens, 2 * width), BF16),
            ((ny, 4 * part, width), BF16), ((ny, 4 * part, width), BF16),
            ((nz, 2 * part, width), BF16), ((nz, 2 * part, width), BF16),
            ((ny, 2 * part, width), BF16), ((ny, 2 * part, width), BF16),
            ((tokens, width), BF16), ((nt, tokens, width), BF16),
            ((nt, own, width), BF16), ((nt, own, width), BF16),
        )
    ] + [
        dma(3), *pair(ny), *pair(nz), *pair(nt), *pair(GATHER_SEMS),
        *pair(ny), *pair(nz), *pair(nz), *pair(ny),
        *pair(ny), *pair(nz), *pair(ny), dma(nx, GATHER_SEMS), dma(nx, GATHER_SEMS), *pair(nt),
    ]
    near = pl.BlockSpec(memory_space=pltpu.VMEM)
    return pl.pallas_call(
        functools.partial(whole_kernel, sizes, ctx_len),
        out_shape=jax.ShapeDtypeStruct((own, d), BF16),
        in_specs=[near] * (len(ins) - 3) + [pl.BlockSpec(memory_space=pl.ANY)] * 3,
        out_specs=near,
        scratch_shapes=scratch,
        compiler_params=pltpu.CompilerParams(
            vmem_limit_bytes=VMEM_LIMIT, collective_id=0, has_side_effects=True
        ),
    )(*ins)


def solution(mesh, ny=8, nz=8, nx=4):
    split = Mesh(mesh.devices.reshape(nz, ny, nx, 2), SP_TP)
    placed = (
        P(SP_TP, None), P(SP, None), P(), P(), P(SP, None, TP), P(), P(None, TP), P(None, TP),
        P(None, TP), P(None, TP), P(TP), P(SP, None),
    )
    return jax.shard_map(
        functools.partial(per_device, (ny, nz, nx)), mesh=split, in_specs=placed,
        out_specs=P(SP_TP, None), check_vma=False,
    )
```

```python
import functools

import jax
import jax.numpy as jnp
import numpy as np
from jax import lax
from jax.experimental import pallas as pl
from jax.experimental.pallas import tpu as pltpu
from jax.sharding import Mesh
from jax.sharding import PartitionSpec as P

HEAD = 64
HALF = HEAD // 2
BLOCK = 128
SP = ("sp_0", "sp_1")
TP = ("tp_0", "tp_1")
SP_TP = SP + TP
EPSILON = 1e-06
ROTARY_BASE = 10000.0
F32, BF16 = jnp.float32, jnp.bfloat16
MESH = pl.DeviceIdType.MESH
VMEM_LIMIT = 60 * 1024 * 1024


def remote(src, dst, send_sem, recv_sem, device):
    return pltpu.make_async_remote_copy(
        src_ref=src, dst_ref=dst, send_sem=send_sem, recv_sem=recv_sem,
        device_id=device, device_id_type=MESH,
    )


def place():
    return {a: lax.axis_index(a) for a in SP_TP}


def tp_peers(at, nx):
    core, x = at["tp_1"], at["tp_0"]
    peers = [{"tp_0": x, "tp_1": 1 - core}]
    for k in range(1, nx):
        there = lax.rem(x + k, nx)
        peers += [{"tp_0": there, "tp_1": core}, {"tp_0": there, "tp_1": 1 - core}]
    return peers


def line_peers(at, axis, n):
    return [{axis: lax.rem(at[axis] + k, n)} for k in range(1, n)]


def greet(peers):
    barrier = pltpu.get_barrier_semaphore()
    for peer in peers:
        pl.semaphore_signal(barrier, inc=1, device_id=peer, device_id_type=MESH)
    return lambda: pl.semaphore_wait(barrier, len(peers))


class Line:
    def __init__(self, at, axis, n, send_sems, recv_sems):
        self.me, self.axis, self.n = at[axis], axis, n
        self.send_sems, self.recv_sems = send_sems, recv_sems
        self.sent = []

    def start(self, source_of, slots):
        for k in range(1, self.n):
            there = lax.rem(self.me + k, self.n)
            copy = remote(
                source_of(there), slots.at[self.me], self.send_sems.at[k],
                self.recv_sems.at[self.me], {self.axis: there},
            )
            copy.start()
            self.sent.append(copy)

    def wait(self, slots):
        for k in range(1, self.n):
            source = lax.rem(self.me + self.n - k, self.n)
            remote(
                slots.at[source], slots.at[source], self.send_sems.at[k],
                self.recv_sems.at[source], {self.axis: source},
            ).wait_recv()

    def drain(self):
        for copy in self.sent:
            copy.wait_send()


class Gather:
    def __init__(self, at, nx, rows, slot, sems):
        self.x, self.core, self.nx, self.rows, self.slot = at["tp_0"], at["tp_1"], nx, rows, slot
        self.send_sems, self.recv_sems = sems
        self.half = rows // 2
        self.sent = []

    def index(self, steps):
        return lax.rem(self.x + self.nx + steps, self.nx)

    def put(self, src, x_of, core_of, first, count, sem, device):
        copy = remote(
            src, self.slot(x_of * 2 + core_of, first, count), self.send_sems.at[sem],
            self.recv_sems.at[sem], device,
        )
        copy.start()
        self.sent.append(copy)

    def came(self, x_of, core_of, first, count, sem):
        view = self.slot(x_of * 2 + core_of, first, count)
        remote(view, view, self.send_sems.at[sem], self.recv_sems.at[sem], {"tp_0": self.x}).wait_recv()

    def start(self, own):
        x, core, h = self.x, self.core, self.half
        right, left = {"tp_0": self.index(1)}, {"tp_0": self.index(-1)}
        self.put(own(0, h), x, core, 0, h, 0, right)
        self.put(own(h, h), x, core, h, h, 2, left)
        self.put(own(h, h), x, core, h, h, 1, right)
        self.put(own(0, h), x, core, 0, h, 3, left)
        self.put(own(0, self.rows), x, core, 0, self.rows, 6, {"tp_1": 1 - core})

    def forward(self):
        core, h = self.core, self.half
        left, right, over = self.index(-1), self.index(1), {"tp_1": 1 - core}
        self.came(left, core, 0, h, 0)
        self.put(self.slot(left * 2 + core, 0, h), left, core, 0, h, 4, {"tp_0": right})
        self.came(right, core, h, h, 2)
        self.put(self.slot(right * 2 + core, h, h), right, core, h, h, 5, {"tp_0": left})
        self.came(left, core, h, h, 1)
        self.put(self.slot(left * 2 + core, 0, self.rows), left, core, 0, self.rows, 7, over)
        self.came(right, core, 0, h, 3)
        self.put(self.slot(right * 2 + core, 0, self.rows), right, core, 0, self.rows, 8, over)

    def finish(self):
        core, h, n = self.core, self.half, self.rows
        far, over = self.index(2), {"tp_1": 1 - core}
        self.came(far, core, 0, h, 4)
        self.came(far, core, h, h, 5)
        self.put(self.slot(far * 2 + core, 0, n), far, core, 0, n, 9, over)
        for sem, steps in ((6, 0), (7, -1), (8, 1), (9, 2)):
            self.came(self.index(steps), 1 - core, 0, n, sem)

    def drain(self):
        for copy in self.sent:
            copy.wait_send()


GATHER_SEMS = 10


def head_masks(heads):
    lane = lax.broadcasted_iota(jnp.int32, (1, heads * HEAD), 1)
    return [(lane >= h * HEAD) & (lane < (h + 1) * HEAD) for h in range(heads)]


def squeezed(full, masks):
    return sum(
        jnp.where(m, full[h * HEAD : (h + 1) * HEAD], 0.0) for h, m in enumerate(masks)
    )


def spread_out(packed, masks):
    return jnp.concatenate([jnp.where(m, packed, 0.0) for m in masks], axis=0)


def rotated(u, cos, sin, low):
    width = u.shape[1]
    partner = jnp.where(low, pltpu.roll(u, width - HALF, 1), pltpu.roll(u, HALF, 1))
    return u * cos + partner * sin


def outer(keys, values):
    return lax.dot_general(
        keys.astype(BF16), values, (((0,), (0,)), ((), ())), preferred_element_type=F32
    )


def averaged(values, average):
    high = values.astype(BF16)
    rest = (values - high.astype(F32)).astype(BF16)
    return jnp.dot(high, average, preferred_element_type=F32) + jnp.dot(
        rest, average, preferred_element_type=F32
    )


def whole_kernel(
    sizes, ctx_len, cond_ref, other_ref, mw_ref, lat_ref, ctx_ref, w_ref, gain_ref, ld_ref, hg_ref,
    cos_ref, sin_ref, base_ref, wq_hbm, wk_hbm, wv_hbm, out_ref,
    wq, wk, wv, part_s, mod, rows_all, stat, normed, cos_s, sin_s, decay,
    ybuf, zbuf, tbuf, ysum, zsum, w_yz, w_zy, wall,
    k_sum, v_sum, k_s, v_s, q_s, u_s, o_s, readers, st, r1, s2, r2, s3, ent, ret, gathered, done, landed,
    wt_sem, y_send, y_recv, z_send, z_recv, t_send, t_recv, l_send, l_recv,
    wa_send, wa_recv, wb_send, wb_recv, wc_send, wc_recv, wd_send, wd_recv,
    a_send, a_recv, b_send, b_recv, c_send, c_recv, g_send, g_recv, o_send, o_recv, x_send, x_recv,
):
    ny, nz, nx = sizes
    nt = 2 * nx
    own, d = lat_ref.shape
    tokens = own * nt
    width = hg_ref.shape[1]
    heads = width // HEAD
    blocks = tokens // BLOCK
    part = HEAD // ny
    ctx_rows = ctx_ref.shape[0]
    at = place()
    y, z, x, core = at["sp_1"], at["sp_0"], at["tp_0"], at["tp_1"]
    t, sp = x * 2 + core, z * ny + y
    tps = tp_peers(at, nx)
    weights = [
        pltpu.make_async_copy(a, b, wt_sem.at[i])
        for i, (a, b) in enumerate(((wk_hbm, wk), (wv_hbm, wv), (wq_hbm, wq)))
    ]
    for copy in weights:
        copy.start()
    met = greet(line_peers(at, "sp_1", ny) + line_peers(at, "sp_0", nz) + tps)

    c = jnp.concatenate([cond_ref[...], other_ref[...], jnp.zeros((6, d), F32)], axis=0)
    activated = (c / (1.0 + jnp.exp(-c))).astype(BF16)
    _, depth, cols = mw_ref.shape
    entry = lax.broadcasted_iota(jnp.int32, (d, depth), 0)
    place_of = lax.broadcasted_iota(jnp.int32, (d, depth), 1) + sp * depth
    mine = jnp.dot(
        activated, jnp.where(entry == place_of, 1.0, 0.0).astype(BF16), preferred_element_type=F32
    ).astype(BF16)
    parts = [jnp.dot(mine, mw_ref[r], preferred_element_type=F32) for r in range(3)]
    part_s[...] = jnp.concatenate(
        [parts[r][k : k + 1] for k in range(2) for r in range(3)] + [parts[0][2:4]], axis=0
    )
    met()
    along_y = Line(at, "sp_1", ny, y_send, y_recv)
    along_z = Line(at, "sp_0", nz, z_send, z_recv)
    along_y.start(lambda there: part_s, ybuf)
    spread_rows = Gather(
        at, nx, own, lambda s, a, n: rows_all.at[pl.ds(s * own + a, n)], (l_send, l_recv)
    )
    spread_rows.start(lambda a, n: lat_ref.at[pl.ds(a, n)])
    ybuf[y] = part_s[...]
    rows_all[pl.ds(pl.multiple_of(t * own, own), own)] = lat_ref[...]
    wrows = w_ref.shape[0]
    w_yz[z, y] = w_ref[:, pl.ds(pl.multiple_of(t * 256, 256), 128)]
    w_zy[y, z] = w_ref[:, pl.ds(pl.multiple_of(t * 256 + 128, 128), 128)]
    wa = Line(at, "sp_1", ny, wa_send, wa_recv)
    wa.start(lambda there: w_yz.at[z, y], w_yz.at[z])
    wb = Line(at, "sp_0", nz, wb_send, wb_recv)
    wb.start(lambda there: w_zy.at[y, z], w_zy.at[y])

    lane = lax.broadcasted_iota(jnp.int32, (1, width), 1)
    low = lax.rem(lane, HEAD) < HALF
    sign = jnp.where(low, -1.0, 1.0)
    repeat = lambda a: jnp.concatenate([a] * (width // a.shape[1]), axis=1)
    base = repeat(base_ref[sp])
    cos_off, sin_off = repeat(cos_ref[...]), repeat(sin_ref[...])
    cos_s[...] = base[0:1] * cos_off - base[1:2] * sin_off
    sin_s[...] = (base[1:2] * cos_off + base[0:1] * sin_off) * sign
    ccos = base[2:3] * cos_off[:ctx_rows] - base[3:4] * sin_off[:ctx_rows]
    csin = (base[3:4] * cos_off[:ctx_rows] + base[2:3] * sin_off[:ctx_rows]) * sign
    masks = head_masks(heads)
    rates = sum(jnp.where(m, ld_ref[:, h : h + 1], 0.0) for h, m in enumerate(masks))
    ldf, ldb = rates[0:1], rates[1:2]
    row = lax.broadcasted_iota(jnp.int32, (BLOCK, BLOCK), 0)
    col = lax.broadcasted_iota(jnp.int32, (BLOCK, BLOCK), 1)
    gap = (row - col).astype(F32)
    for h in range(heads):
        f, b = ldf[:, h * HEAD : h * HEAD + 1], ldb[:, h * HEAD : h * HEAD + 1]
        decay[h * BLOCK : (h + 1) * BLOCK] = jnp.where(
            gap >= 0, jnp.exp(f * jnp.maximum(gap, 0.0)), 0.0
        ) + jnp.where(gap <= 0, jnp.exp(b * jnp.maximum(-gap, 0.0)), 0.0)

    along_y.wait(ybuf)
    ysum[...] = sum(ybuf[k] for k in range(ny))
    along_z.start(lambda there: ysum, zbuf)
    zbuf[z] = ysum[...]
    wb.wait(w_zy.at[y])
    wd = Line(at, "sp_1", ny, wd_send, wd_recv)
    wd.start(lambda there: w_zy.at[y], w_zy)
    spread_rows.forward()
    along_z.wait(zbuf)
    zsum[...] = sum(zbuf[k] for k in range(nz))
    sent = []
    for k, peer in enumerate(tps):
        copy = remote(zsum, tbuf.at[t], t_send.at[k], t_recv.at[t], peer)
        copy.start()
        sent.append(copy)
    tbuf[t] = zsum[...]
    wa.wait(w_yz.at[z])
    wc = Line(at, "sp_0", nz, wc_send, wc_recv)
    wc.start(lambda there: w_yz.at[z], w_yz)
    spread_rows.finish()

    def root(rows):
        wide = rows.astype(F32)
        return lax.rsqrt(jnp.mean(wide * wide, axis=-1, keepdims=True) + EPSILON)

    @pl.loop(0, tokens // 64)
    def _(i):
        rows = pl.ds(pl.multiple_of(i * 64, 64), 64)
        stat[rows] = jnp.broadcast_to(root(rows_all[rows]), (64, 128))

    ctx_root = root(ctx_ref[...])

    def came(s):
        remote(
            tbuf.at[s], tbuf.at[s], t_send.at[0], t_recv.at[s], {"tp_1": 1 - core}
        ).wait_recv()

    def norm(rows, r, k, columns):
        scale = gain_ref[:, columns] * (1.0 + mod[3 * k + 1 : 3 * k + 2, columns])
        return (rows.astype(F32) * r * scale + mod[3 * k : 3 * k + 1, columns]).astype(BF16)

    for steps in (0, 1, 3, 2):
        chip = lax.rem(x + steps, nx)
        came(2 * chip + 1 - core)
        if steps:
            came(2 * chip + core)
        for k in range(2):
            columns = pl.ds(pl.multiple_of(chip * 512 + k * 256, 256), 256)
            mod[:, columns] = tbuf[2 * chip + k]
        if steps == 0:
            weights[0].wait()
            weights[1].wait()
        for k in range(2):
            columns = pl.ds(pl.multiple_of(chip * 512 + k * 256, 256), 256)
            r = jnp.concatenate([stat[...]] * 2, axis=1)
            normed[0:tokens, columns] = norm(rows_all[:, columns], r, 0, columns)
            normed[tokens : tokens + ctx_rows, columns] = norm(
                ctx_ref[:, columns], ctx_root, 1, columns
            )
        columns = pl.ds(pl.multiple_of(chip * 512, 512), 512)
        k_more = jnp.dot(normed[:, columns], wk[columns], preferred_element_type=F32)
        v_more = jnp.dot(normed[:, columns], wv[columns], preferred_element_type=F32)
        if steps == 0:
            k_sum[...] = k_more
            v_sum[...] = v_more
        elif steps != 2:
            k_sum[...] += k_more
            v_sum[...] += v_more
        else:
            k_all = k_sum[...] + k_more
            v_all = (v_sum[...] + v_more).astype(BF16)
    v_s[...] = v_all[:tokens]
    k_s[...] = rotated(k_all[:tokens], cos_s[...], sin_s[...], low).astype(BF16)
    ck = rotated(k_all[tokens:], ccos, csin, low).astype(BF16).astype(F32)
    cv = v_all[tokens:]
    spot = (sp * ctx_rows + lax.broadcasted_iota(jnp.int32, (ctx_rows, 1), 0)).astype(F32)
    cf = squeezed(outer(ck * jnp.exp(ldf * (ctx_len - 1.0 - spot)), cv), masks)
    cb = squeezed(outer(ck * jnp.exp(ldb * spot), cv), masks)
    l = lax.broadcasted_iota(jnp.int32, (BLOCK, 1), 0).astype(F32)
    to_end, to_start = jnp.exp(ldf * (BLOCK - 1.0 - l)), jnp.exp(ldb * l)
    gf, gb = jnp.exp(ldf * BLOCK), jnp.exp(ldb * BLOCK)
    sf = jnp.zeros((HEAD, width), F32)
    ub = []
    for b in range(blocks):
        keys = k_s[b * BLOCK : (b + 1) * BLOCK].astype(F32)
        values = v_s[b * BLOCK : (b + 1) * BLOCK]
        u_s[b] = sf
        sf = gf * sf + squeezed(outer(keys * to_end, values), masks)
        ub.append(squeezed(outer(keys * to_start, values), masks))
    sb = jnp.zeros((HEAD, width), F32)
    for b in reversed(range(blocks)):
        u_s[blocks + b] = sb
        sb = gb * sb + ub[b]
    for s in range(ny):
        rows = slice(s * part, (s + 1) * part)
        st[s] = jnp.concatenate([sf[rows], sb[rows], cf[rows], cb[rows]], axis=0).astype(BF16)
    one = Line(at, "sp_1", ny, a_send, a_recv)
    one.start(lambda there: st.at[there], r1)
    r1[y] = st[y]

    weights[2].wait()
    q_all = jnp.dot(normed[0:tokens], wq[...], preferred_element_type=F32)
    queries = (rotated(q_all, cos_s[...], sin_s[...], low) * HEAD ** (-0.5)).astype(BF16)
    read_f, read_b = jnp.exp(ldf * (l + 1.0)), jnp.exp(ldb * (BLOCK - l))
    q_s[...] = queries

    def near(i):
        rows = slice(i * BLOCK, (i + 1) * BLOCK)
        wide = q_s[rows].astype(F32)
        stacked = jnp.concatenate([jnp.where(m, wide, 0.0) for m in masks], axis=0).astype(BF16)
        scores = lax.dot_general(
            stacked, k_s[rows], (((1,), (1,)), ((), ())), preferred_element_type=F32
        )
        inside = jnp.dot(
            (scores * decay[...]).astype(BF16), v_s[rows], preferred_element_type=F32
        )
        states = jnp.concatenate(
            [spread_out(u_s[i], masks), spread_out(u_s[blocks + i], masks)], axis=0
        ).astype(BF16)
        near_f, near_b = wide * read_f, wide * read_b
        o = jnp.dot(
            jnp.concatenate([near_f, near_b], axis=1).astype(BF16), states,
            preferred_element_type=F32,
        )
        for h, m in enumerate(masks):
            o = o + jnp.where(m, inside[h * BLOCK : (h + 1) * BLOCK], 0.0)
        o_s[rows] = o
        far_f = wide * jnp.exp(ldf * (l + (i * BLOCK + 1.0)))
        far_b = wide * jnp.exp(ldb * ((tokens - i * BLOCK) - l))
        readers[rows] = jnp.concatenate([far_f, far_b], axis=1).astype(BF16)

    for i in range(blocks // 2):
        near(i)
    one.wait(r1)
    got = [r1[j].astype(F32) for j in range(ny)]
    hf, hb = jnp.exp(ldf * tokens), jnp.exp(ldb * tokens)
    ahead = [jnp.zeros_like(got[0][:part])]
    for j in range(ny):
        ahead.append(hf * ahead[-1] + got[j][:part])
    total_f = ahead.pop()
    behind = [jnp.zeros_like(ahead[0])]
    for j in reversed(range(ny)):
        behind.append(hb * behind[-1] + got[j][part : 2 * part])
    total_b = behind.pop()
    behind = behind[::-1]
    ctx = sum(got)
    ctx_f, ctx_b = ctx[2 * part : 3 * part], ctx[3 * part :]
    span = float(tokens * ny)
    for k in range(nz):
        there = lax.rem(z + k, nz)
        ahead_by = (there - z).astype(F32)
        to_f = jnp.where(there > z, 1.0, 0.0) * jnp.exp(ldf * (span * jnp.maximum(ahead_by - 1.0, 0.0)))
        to_b = jnp.where(there < z, 1.0, 0.0) * jnp.exp(ldb * (span * jnp.maximum(-ahead_by - 1.0, 0.0)))
        start_f = jnp.exp(ldf * (span * there.astype(F32)))
        start_b = jnp.exp(ldb * (span * (nz - 1 - there).astype(F32)))
        s2[there] = jnp.concatenate(
            [to_f * total_f + start_f * ctx_f, to_b * total_b + start_b * ctx_b], axis=0
        ).astype(BF16)
    two = Line(at, "sp_0", nz, b_send, b_recv)
    two.start(lambda there: s2.at[there], r2)
    r2[z] = s2[z]
    for i in range(blocks // 2, blocks):
        near(i)
    wc.wait(w_yz)
    two.wait(r2)
    entering = sum(r2[j].astype(F32) for j in range(nz))
    for j in range(ny):
        s3[j] = jnp.concatenate(
            [
                ahead[j] + jnp.exp(ldf * float(tokens * j)) * entering[:part],
                behind[j] + jnp.exp(ldb * float(tokens * (ny - 1 - j))) * entering[part:],
            ],
            axis=0,
        ).astype(BF16)
    three = Line(at, "sp_1", ny, c_send, c_recv)
    three.start(lambda there: s3.at[there], ent)
    ent[y] = s3[y]
    wd.wait(w_zy)
    for a in range(nz):
        for b in range(ny):
            first = (a * ny + b) * wrows
            wall[core, first : first + wrows, 0:128] = w_yz[a, b]
            wall[core, first : first + wrows, 128:256] = w_zy[b, a]
    over = {"tp_1": 1 - core}
    w_over = remote(wall.at[core], wall.at[core], x_send.at[0], x_recv.at[0], over)
    w_over.start()
    a = lax.broadcasted_iota(jnp.int32, (width, width), 0)
    b = lax.broadcasted_iota(jnp.int32, (width, width), 1)
    average = jnp.where(a // HEAD == b // HEAD, 1.0 / HEAD, 0.0).astype(BF16)
    three.wait(ent)

    slices = [ent[s].astype(F32) for s in range(ny)]
    states = jnp.concatenate(
        [
            spread_out(jnp.concatenate([e[:part] for e in slices], axis=0), masks),
            spread_out(jnp.concatenate([e[part:] for e in slices], axis=0), masks),
        ],
        axis=0,
    ).astype(BF16)
    order = (2, 1, 3, 0)
    right, left = lax.rem(x + 1, nx), lax.rem(x + nx - 1, nx)
    to_right, to_left = {"tp_0": right}, {"tp_0": left}
    partner = t + 1 - 2 * core
    posted = []

    def post(src, dst, q, s, r, device):
        copy = remote(src, dst, g_send.at[q, s], g_recv.at[q, r], device)
        copy.start()
        posted.append(copy)

    def arrived(q, s, r):
        remote(
            gathered.at[q, s], gathered.at[q, s], g_send.at[q, 0], g_recv.at[q, r], over
        ).wait_recv()

    for steps in order:
        q = lax.rem(x + steps, nx)
        rows = pl.ds(pl.multiple_of(q * 2 * own, 2 * own), 2 * own)
        o = o_s[rows] + jnp.dot(readers[rows], states, preferred_element_type=F32)
        centred = o - averaged(o, average)
        spread = averaged(centred * centred, average)
        kept = (centred * lax.rsqrt(spread + EPSILON) * hg_ref[...]).astype(BF16)
        ret[2 * q] = kept[:own]
        ret[2 * q + 1] = kept[own:]
        post(ret.at[2 * q + 1 - core], gathered.at[q, t], q, 0, 0, over)
        post(ret.at[2 * q + core], gathered.at[q, t], q, 1, 1 + core, to_right)
        post(ret.at[2 * q + core], gathered.at[q, t], q, 2, 3 + core, to_left)
        gathered[q, t] = ret[2 * q + core]
    for steps in order:
        q = lax.rem(x + steps, nx)
        arrived(q, partner, 0)
        post(gathered.at[q, partner], gathered.at[q, partner], q, 3, 2 - core, to_right)
        post(gathered.at[q, partner], gathered.at[q, partner], q, 4, 4 - core, to_left)
        q = lax.rem(left + steps, nx)
        arrived(q, 2 * left, 1)
        post(gathered.at[q, 2 * left], gathered.at[q, 2 * left], q, 5, 5, to_right)
        q = lax.rem(right + steps, nx)
        arrived(q, 2 * right + 1, 4)
        post(gathered.at[q, 2 * right + 1], gathered.at[q, 2 * right + 1], q, 6, 6, to_left)
    w_over.wait_recv()
    far = lax.rem(x + 2, nx)

    def mixed_for(qs):
        for q in qs:
            arrived(q, 2 * left + 1, 2)
            arrived(q, 2 * right, 3)
            arrived(q, 2 * far, 5)
            arrived(q, 2 * far + 1, 6)
        rows = jnp.concatenate(
            [jnp.concatenate([gathered[q, s] for s in range(nt)], axis=1) for q in qs], axis=0
        )
        for k in range(2):
            columns = pl.ds(pl.multiple_of((2 * x + k) * width, width), width)
            mixed = jnp.dot(rows, wall[k], preferred_element_type=F32)
            for i, q in enumerate(qs):
                mine = pl.ds(pl.multiple_of((2 * q + core) * own, own), own)
                result = rows_all[mine, columns].astype(F32) + mod[2:3, columns] * mixed[
                    i * own : (i + 1) * own
                ]
                done[q, :, k * width : (k + 1) * width] = result.astype(BF16)

    def give(steps):
        q = lax.rem(x + steps, nx)
        copy = remote(done.at[q], landed.at[x], o_send.at[steps], o_recv.at[x], {"tp_0": q})
        copy.start()
        posted.append(copy)

    mixed_for([far])
    give(2)
    mixed_for([right, left])
    give(1)
    give(nx - 1)
    mixed_for([x])
    landed[x] = done[x]
    for chip in (right, left, far):
        remote(
            landed.at[chip], landed.at[chip], o_send.at[0], o_recv.at[chip], {"tp_0": chip}
        ).wait_recv()
    for chip in range(nx):
        out_ref[:, chip * 2 * width : (chip + 1) * 2 * width] = landed[chip]
    for line in (along_y, along_z, wa, wb, wc, wd, one, two, three, spread_rows):
        line.drain()
    for copy in sent + posted + [w_over]:
        copy.wait_send()


def turns(positions):
    frequency = ROTARY_BASE ** -np.linspace(0.0, 1.0, HALF)
    angles = np.asarray(positions, np.float64)[:, None] * frequency[None]
    tile = lambda a: np.tile(np.asarray(a, np.float32), (1, 128 // HALF))
    return tile(np.cos(angles)), tile(np.sin(angles))


def per_device(
    sizes, latent, context, condition, context_condition, modulation_weight, norm_gain,
    query_weight, key_weight, value_weight, log_decay, head_gain, output_weight,
):
    ny, nz, nx = sizes
    nt = 2 * nx
    d = latent.shape[1]
    width = query_weight.shape[1]
    heads = width // HEAD
    own = latent.shape[0]
    tokens = own * nt
    ctx_rows = context.shape[0]
    ctx_len = ctx_rows * ny * nz
    wrows = output_weight.shape[0]
    cos_off, sin_off = turns(np.arange(tokens))
    bases = np.stack(
        turns(ctx_len + tokens * np.arange(ny * nz)) + turns(ctx_rows * np.arange(ny * nz)), axis=1
    )
    ins = [
        condition.reshape(1, d), context_condition.reshape(1, d),
        modulation_weight.transpose(1, 0, 2), latent, context, output_weight, norm_gain.reshape(1, d),
        log_decay, head_gain.reshape(1, width), jnp.asarray(cos_off), jnp.asarray(sin_off),
        jnp.asarray(bases), query_weight, key_weight, value_weight,
    ]
    dma = lambda *n: pltpu.SemaphoreType.DMA(n)
    part, blocks = HEAD // ny, tokens // BLOCK
    pair = lambda n: [dma(n), dma(n)]
    scratch = [
        pltpu.VMEM(shape, kind)
        for shape, kind in (
            *[((d, width), BF16)] * 3,
            ((8, width), F32), ((8, d), F32), ((tokens, d), BF16), ((tokens, 128), F32),
            ((tokens + ctx_rows, d), BF16), ((tokens, width), F32), ((tokens, width), F32),
            ((heads * BLOCK, BLOCK), F32),
            ((ny, 8, width), F32), ((nz, 8, width), F32), ((nt, 8, width), F32),
            ((8, width), F32), ((8, width), F32),
            ((nz, ny, wrows, 128), BF16), ((ny, nz, wrows, 128), BF16), ((2, d, width), BF16),
            ((tokens + ctx_rows, width), F32), ((tokens + ctx_rows, width), F32),
            ((tokens, width), BF16), ((tokens, width), BF16), ((tokens, width), BF16),
            ((2 * blocks, HEAD, width), F32),
            ((tokens, width), F32), ((tokens, 2 * width), BF16),
            ((ny, 4 * part, width), BF16), ((ny, 4 * part, width), BF16),
            ((nz, 2 * part, width), BF16), ((nz, 2 * part, width), BF16),
            ((ny, 2 * part, width), BF16), ((ny, 2 * part, width), BF16),
            ((nt, own, width), BF16), ((nx, nt, own, width), BF16),
            ((nx, own, 2 * width), BF16), ((nx, own, 2 * width), BF16),
        )
    ] + [
        dma(3), *pair(ny), *pair(nz), *pair(nt), *pair(GATHER_SEMS),
        *pair(ny), *pair(nz), *pair(nz), *pair(ny),
        *pair(ny), *pair(nz), *pair(ny), dma(nx, 7), dma(nx, 7), *pair(nx), *pair(1),
    ]
    near = pl.BlockSpec(memory_space=pltpu.VMEM)
    return pl.pallas_call(
        functools.partial(whole_kernel, sizes, ctx_len),
        out_shape=jax.ShapeDtypeStruct((own, d), BF16),
        in_specs=[near] * (len(ins) - 3) + [pl.BlockSpec(memory_space=pl.ANY)] * 3,
        out_specs=near,
        scratch_shapes=scratch,
        compiler_params=pltpu.CompilerParams(
            vmem_limit_bytes=VMEM_LIMIT, collective_id=0, has_side_effects=True
        ),
    )(*ins)


def solution(mesh, ny=8, nz=8, nx=4):
    split = Mesh(mesh.devices.reshape(nz, ny, nx, 2), SP_TP)
    placed = (
        P(SP_TP, None), P(SP, None), P(), P(), P(SP, None, TP), P(), P(None, TP), P(None, TP),
        P(None, TP), P(None, TP), P(TP), P(SP, None),
    )
    return jax.shard_map(
        functools.partial(per_device, (ny, nz, nx)), mesh=split, in_specs=placed,
        out_specs=P(SP_TP, None), check_vma=False,
    )
```

```python
import functools

import jax
import jax.numpy as jnp
import numpy as np
from jax import lax
from jax.experimental import pallas as pl
from jax.experimental.pallas import tpu as pltpu
from jax.sharding import Mesh
from jax.sharding import PartitionSpec as P

HEAD = 64
HALF = HEAD // 2
BLOCK = 128
SP = ("sp_0", "sp_1")
TP = ("tp_0", "tp_1")
SP_TP = SP + TP
EPSILON = 1e-06
ROTARY_BASE = 10000.0
F32, BF16 = jnp.float32, jnp.bfloat16
MESH = pl.DeviceIdType.MESH
VMEM_LIMIT = 60 * 1024 * 1024


def remote(src, dst, send_sem, recv_sem, device):
    return pltpu.make_async_remote_copy(
        src_ref=src, dst_ref=dst, send_sem=send_sem, recv_sem=recv_sem,
        device_id=device, device_id_type=MESH,
    )


def place():
    return {a: lax.axis_index(a) for a in SP_TP}


def tp_peers(at, nx):
    core, x = at["tp_1"], at["tp_0"]
    peers = [{"tp_0": x, "tp_1": 1 - core}]
    for k in range(1, nx):
        there = lax.rem(x + k, nx)
        peers += [{"tp_0": there, "tp_1": core}, {"tp_0": there, "tp_1": 1 - core}]
    return peers


def line_peers(at, axis, n):
    return [{axis: lax.rem(at[axis] + k, n)} for k in range(1, n)]


def greet(peers):
    barrier = pltpu.get_barrier_semaphore()
    for peer in peers:
        pl.semaphore_signal(barrier, inc=1, device_id=peer, device_id_type=MESH)
    return lambda: pl.semaphore_wait(barrier, len(peers))


class Line:
    def __init__(self, at, axis, n, send_sems, recv_sems):
        self.me, self.axis, self.n = at[axis], axis, n
        self.send_sems, self.recv_sems = send_sems, recv_sems
        self.sent = []

    def start(self, source_of, slots):
        for k in range(1, self.n):
            there = lax.rem(self.me + k, self.n)
            copy = remote(
                source_of(there), slots.at[self.me], self.send_sems.at[k],
                self.recv_sems.at[self.me], {self.axis: there},
            )
            copy.start()
            self.sent.append(copy)

    def wait(self, slots):
        for k in range(1, self.n):
            source = lax.rem(self.me + self.n - k, self.n)
            remote(
                slots.at[source], slots.at[source], self.send_sems.at[k],
                self.recv_sems.at[source], {self.axis: source},
            ).wait_recv()

    def drain(self):
        for copy in self.sent:
            copy.wait_send()


class Gather:
    def __init__(self, at, nx, rows, slot, sems):
        self.x, self.core, self.nx, self.rows, self.slot = at["tp_0"], at["tp_1"], nx, rows, slot
        self.send_sems, self.recv_sems = sems
        self.half = rows // 2
        self.sent = []

    def index(self, steps):
        return lax.rem(self.x + self.nx + steps, self.nx)

    def put(self, src, x_of, core_of, first, count, sem, device):
        copy = remote(
            src, self.slot(x_of * 2 + core_of, first, count), self.send_sems.at[sem],
            self.recv_sems.at[sem], device,
        )
        copy.start()
        self.sent.append(copy)

    def came(self, x_of, core_of, first, count, sem):
        view = self.slot(x_of * 2 + core_of, first, count)
        remote(view, view, self.send_sems.at[sem], self.recv_sems.at[sem], {"tp_0": self.x}).wait_recv()

    def start(self, own):
        x, core, h = self.x, self.core, self.half
        right, left = {"tp_0": self.index(1)}, {"tp_0": self.index(-1)}
        self.put(own(0, h), x, core, 0, h, 0, right)
        self.put(own(h, h), x, core, h, h, 2, left)
        self.put(own(h, h), x, core, h, h, 1, right)
        self.put(own(0, h), x, core, 0, h, 3, left)
        self.put(own(0, self.rows), x, core, 0, self.rows, 6, {"tp_1": 1 - core})

    def forward(self):
        core, h = self.core, self.half
        left, right, over = self.index(-1), self.index(1), {"tp_1": 1 - core}
        self.came(left, core, 0, h, 0)
        self.put(self.slot(left * 2 + core, 0, h), left, core, 0, h, 4, {"tp_0": right})
        self.came(right, core, h, h, 2)
        self.put(self.slot(right * 2 + core, h, h), right, core, h, h, 5, {"tp_0": left})
        self.came(left, core, h, h, 1)
        self.put(self.slot(left * 2 + core, 0, self.rows), left, core, 0, self.rows, 7, over)
        self.came(right, core, 0, h, 3)
        self.put(self.slot(right * 2 + core, 0, self.rows), right, core, 0, self.rows, 8, over)

    def finish(self):
        core, h, n = self.core, self.half, self.rows
        far, over = self.index(2), {"tp_1": 1 - core}
        self.came(far, core, 0, h, 4)
        self.came(far, core, h, h, 5)
        self.put(self.slot(far * 2 + core, 0, n), far, core, 0, n, 9, over)
        for sem, steps in ((6, 0), (7, -1), (8, 1), (9, 2)):
            self.came(self.index(steps), 1 - core, 0, n, sem)

    def drain(self):
        for copy in self.sent:
            copy.wait_send()


GATHER_SEMS = 10


def head_masks(heads):
    lane = lax.broadcasted_iota(jnp.int32, (1, heads * HEAD), 1)
    return [(lane >= h * HEAD) & (lane < (h + 1) * HEAD) for h in range(heads)]


def squeezed(full, masks):
    return sum(
        jnp.where(m, full[h * HEAD : (h + 1) * HEAD], 0.0) for h, m in enumerate(masks)
    )


def spread_out(packed, masks):
    return jnp.concatenate([jnp.where(m, packed, 0.0) for m in masks], axis=0)


def rotated(u, cos, sin, low):
    width = u.shape[1]
    partner = jnp.where(low, pltpu.roll(u, width - HALF, 1), pltpu.roll(u, HALF, 1))
    return u * cos + partner * sin


def outer(keys, values):
    return lax.dot_general(
        keys.astype(BF16), values, (((0,), (0,)), ((), ())), preferred_element_type=F32
    )


def averaged(values, average):
    high = values.astype(BF16)
    rest = (values - high.astype(F32)).astype(BF16)
    return jnp.dot(high, average, preferred_element_type=F32) + jnp.dot(
        rest, average, preferred_element_type=F32
    )


def whole_kernel(
    sizes, ctx_len, cond_ref, other_ref, mw_ref, lat_ref, ctx_ref, w_ref, gain_ref, ld_ref, hg_ref,
    cos_ref, sin_ref, base_ref, wq_hbm, wk_hbm, wv_hbm, out_ref,
    wq, wk, wv, part_s, mod, rows_all, stat, normed, cos_s, sin_s, decay,
    ybuf, zbuf, tbuf, ysum, zsum, w_yz, w_zy, wall,
    k_sum, v_sum, k_s, v_s, q_s, u_s, o_s, readers, st, r1, s2, r2, s3, ent, ret, gathered, done, landed,
    wt_sem, y_send, y_recv, z_send, z_recv, t_send, t_recv, l_send, l_recv,
    wa_send, wa_recv, wb_send, wb_recv, wc_send, wc_recv, wd_send, wd_recv,
    a_send, a_recv, b_send, b_recv, c_send, c_recv, g_send, g_recv, o_send, o_recv, x_send, x_recv,
):
    ny, nz, nx = sizes
    nt = 2 * nx
    own, d = lat_ref.shape
    tokens = own * nt
    width = hg_ref.shape[1]
    heads = width // HEAD
    blocks = tokens // BLOCK
    part = HEAD // ny
    ctx_rows = ctx_ref.shape[0]
    at = place()
    y, z, x, core = at["sp_1"], at["sp_0"], at["tp_0"], at["tp_1"]
    t, sp = x * 2 + core, z * ny + y
    tps = tp_peers(at, nx)
    weights = [
        pltpu.make_async_copy(a, b, wt_sem.at[i])
        for i, (a, b) in enumerate(((wk_hbm, wk), (wv_hbm, wv), (wq_hbm, wq)))
    ]
    for copy in weights:
        copy.start()
    met = greet(line_peers(at, "sp_1", ny) + line_peers(at, "sp_0", nz) + tps)

    c = jnp.concatenate([cond_ref[...], other_ref[...], jnp.zeros((6, d), F32)], axis=0)
    activated = (c / (1.0 + jnp.exp(-c))).astype(BF16)
    _, depth, cols = mw_ref.shape
    entry = lax.broadcasted_iota(jnp.int32, (d, depth), 0)
    place_of = lax.broadcasted_iota(jnp.int32, (d, depth), 1) + sp * depth
    mine = jnp.dot(
        activated, jnp.where(entry == place_of, 1.0, 0.0).astype(BF16), preferred_element_type=F32
    ).astype(BF16)
    parts = [jnp.dot(mine, mw_ref[r], preferred_element_type=F32) for r in range(3)]
    part_s[...] = jnp.concatenate(
        [parts[r][k : k + 1] for k in range(2) for r in range(3)] + [parts[0][2:4]], axis=0
    )
    met()
    along_y = Line(at, "sp_1", ny, y_send, y_recv)
    along_z = Line(at, "sp_0", nz, z_send, z_recv)
    along_y.start(lambda there: part_s, ybuf)
    spread_rows = Gather(
        at, nx, own, lambda s, a, n: rows_all.at[pl.ds(s * own + a, n)], (l_send, l_recv)
    )
    spread_rows.start(lambda a, n: lat_ref.at[pl.ds(a, n)])
    ybuf[y] = part_s[...]
    rows_all[pl.ds(pl.multiple_of(t * own, own), own)] = lat_ref[...]
    wrows = w_ref.shape[0]
    w_yz[z, y] = w_ref[:, pl.ds(pl.multiple_of(t * 256, 256), 128)]
    w_zy[y, z] = w_ref[:, pl.ds(pl.multiple_of(t * 256 + 128, 128), 128)]
    wa = Line(at, "sp_1", ny, wa_send, wa_recv)
    wa.start(lambda there: w_yz.at[z, y], w_yz.at[z])
    wb = Line(at, "sp_0", nz, wb_send, wb_recv)
    wb.start(lambda there: w_zy.at[y, z], w_zy.at[y])

    lane = lax.broadcasted_iota(jnp.int32, (1, width), 1)
    low = lax.rem(lane, HEAD) < HALF
    sign = jnp.where(low, -1.0, 1.0)
    repeat = lambda a: jnp.concatenate([a] * (width // a.shape[1]), axis=1)
    base = repeat(base_ref[sp])
    cos_off, sin_off = repeat(cos_ref[...]), repeat(sin_ref[...])
    cos_s[...] = base[0:1] * cos_off - base[1:2] * sin_off
    sin_s[...] = (base[1:2] * cos_off + base[0:1] * sin_off) * sign
    ccos = base[2:3] * cos_off[:ctx_rows] - base[3:4] * sin_off[:ctx_rows]
    csin = (base[3:4] * cos_off[:ctx_rows] + base[2:3] * sin_off[:ctx_rows]) * sign
    masks = head_masks(heads)
    rates = sum(jnp.where(m, ld_ref[:, h : h + 1], 0.0) for h, m in enumerate(masks))
    ldf, ldb = rates[0:1], rates[1:2]
    row = lax.broadcasted_iota(jnp.int32, (BLOCK, BLOCK), 0)
    col = lax.broadcasted_iota(jnp.int32, (BLOCK, BLOCK), 1)
    gap = (row - col).astype(F32)
    for h in range(heads):
        f, b = ldf[:, h * HEAD : h * HEAD + 1], ldb[:, h * HEAD : h * HEAD + 1]
        decay[h * BLOCK : (h + 1) * BLOCK] = jnp.where(
            gap >= 0, jnp.exp(f * jnp.maximum(gap, 0.0)), 0.0
        ) + jnp.where(gap <= 0, jnp.exp(b * jnp.maximum(-gap, 0.0)), 0.0)

    along_y.wait(ybuf)
    ysum[...] = sum(ybuf[k] for k in range(ny))
    along_z.start(lambda there: ysum, zbuf)
    zbuf[z] = ysum[...]
    wb.wait(w_zy.at[y])
    wd = Line(at, "sp_1", ny, wd_send, wd_recv)
    wd.start(lambda there: w_zy.at[y], w_zy)
    spread_rows.forward()
    along_z.wait(zbuf)
    zsum[...] = sum(zbuf[k] for k in range(nz))
    sent = []
    for k, peer in enumerate(tps):
        copy = remote(zsum, tbuf.at[t], t_send.at[k], t_recv.at[t], peer)
        copy.start()
        sent.append(copy)
    tbuf[t] = zsum[...]
    wa.wait(w_yz.at[z])
    wc = Line(at, "sp_0", nz, wc_send, wc_recv)
    wc.start(lambda there: w_yz.at[z], w_yz)
    spread_rows.finish()

    def root(rows):
        wide = rows.astype(F32)
        return lax.rsqrt(jnp.mean(wide * wide, axis=-1, keepdims=True) + EPSILON)

    @pl.loop(0, tokens // 64)
    def _(i):
        rows = pl.ds(pl.multiple_of(i * 64, 64), 64)
        stat[rows] = jnp.broadcast_to(root(rows_all[rows]), (64, 128))

    ctx_root = root(ctx_ref[...])

    def came(s):
        remote(
            tbuf.at[s], tbuf.at[s], t_send.at[0], t_recv.at[s], {"tp_1": 1 - core}
        ).wait_recv()

    def norm(rows, r, k, columns):
        scale = gain_ref[:, columns] * (1.0 + mod[3 * k + 1 : 3 * k + 2, columns])
        return (rows.astype(F32) * r * scale + mod[3 * k : 3 * k + 1, columns]).astype(BF16)

    for steps in (0, 1, 3, 2):
        chip = lax.rem(x + steps, nx)
        came(2 * chip + 1 - core)
        if steps:
            came(2 * chip + core)
        for k in range(2):
            columns = pl.ds(pl.multiple_of(chip * 512 + k * 256, 256), 256)
            mod[:, columns] = tbuf[2 * chip + k]
        if steps == 0:
            weights[0].wait()
            weights[1].wait()
        for k in range(2):
            columns = pl.ds(pl.multiple_of(chip * 512 + k * 256, 256), 256)
            r = jnp.concatenate([stat[...]] * 2, axis=1)
            normed[0:tokens, columns] = norm(rows_all[:, columns], r, 0, columns)
            normed[tokens : tokens + ctx_rows, columns] = norm(
                ctx_ref[:, columns], ctx_root, 1, columns
            )
        columns = pl.ds(pl.multiple_of(chip * 512, 512), 512)
        k_more = jnp.dot(normed[:, columns], wk[columns], preferred_element_type=F32)
        v_more = jnp.dot(normed[:, columns], wv[columns], preferred_element_type=F32)
        if steps == 0:
            k_sum[...] = k_more
            v_sum[...] = v_more
        elif steps != 2:
            k_sum[...] += k_more
            v_sum[...] += v_more
        else:
            k_all = k_sum[...] + k_more
            v_all = (v_sum[...] + v_more).astype(BF16)
    v_s[...] = v_all[:tokens]
    k_s[...] = rotated(k_all[:tokens], cos_s[...], sin_s[...], low).astype(BF16)
    ck = rotated(k_all[tokens:], ccos, csin, low).astype(BF16).astype(F32)
    cv = v_all[tokens:]
    spot = (sp * ctx_rows + lax.broadcasted_iota(jnp.int32, (ctx_rows, 1), 0)).astype(F32)
    cf = squeezed(outer(ck * jnp.exp(ldf * (ctx_len - 1.0 - spot)), cv), masks)
    cb = squeezed(outer(ck * jnp.exp(ldb * spot), cv), masks)
    l = lax.broadcasted_iota(jnp.int32, (BLOCK, 1), 0).astype(F32)
    to_end, to_start = jnp.exp(ldf * (BLOCK - 1.0 - l)), jnp.exp(ldb * l)
    gf, gb = jnp.exp(ldf * BLOCK), jnp.exp(ldb * BLOCK)
    sf = jnp.zeros((HEAD, width), F32)
    ub = []
    for b in range(blocks):
        keys = k_s[b * BLOCK : (b + 1) * BLOCK].astype(F32)
        values = v_s[b * BLOCK : (b + 1) * BLOCK]
        u_s[b] = sf
        sf = gf * sf + squeezed(outer(keys * to_end, values), masks)
        ub.append(squeezed(outer(keys * to_start, values), masks))
    sb = jnp.zeros((HEAD, width), F32)
    for b in reversed(range(blocks)):
        u_s[blocks + b] = sb
        sb = gb * sb + ub[b]
    for s in range(ny):
        rows = slice(s * part, (s + 1) * part)
        st[s] = jnp.concatenate([sf[rows], sb[rows], cf[rows], cb[rows]], axis=0).astype(BF16)
    one = Line(at, "sp_1", ny, a_send, a_recv)
    one.start(lambda there: st.at[there], r1)
    r1[y] = st[y]

    weights[2].wait()
    q_all = jnp.dot(normed[0:tokens], wq[...], preferred_element_type=F32)
    queries = (rotated(q_all, cos_s[...], sin_s[...], low) * HEAD ** (-0.5)).astype(BF16)
    read_f, read_b = jnp.exp(ldf * (l + 1.0)), jnp.exp(ldb * (BLOCK - l))
    a = lax.broadcasted_iota(jnp.int32, (width, width), 0)
    b = lax.broadcasted_iota(jnp.int32, (width, width), 1)
    average = jnp.where(a // HEAD == b // HEAD, 1.0 / HEAD, 0.0).astype(BF16)
    q_s[...] = queries

    def near(i):
        rows = slice(i * BLOCK, (i + 1) * BLOCK)
        wide = q_s[rows].astype(F32)
        stacked = jnp.concatenate([jnp.where(m, wide, 0.0) for m in masks], axis=0).astype(BF16)
        scores = lax.dot_general(
            stacked, k_s[rows], (((1,), (1,)), ((), ())), preferred_element_type=F32
        )
        inside = jnp.dot(
            (scores * decay[...]).astype(BF16), v_s[rows], preferred_element_type=F32
        )
        states = jnp.concatenate(
            [spread_out(u_s[i], masks), spread_out(u_s[blocks + i], masks)], axis=0
        ).astype(BF16)
        near_f, near_b = wide * read_f, wide * read_b
        o = jnp.dot(
            jnp.concatenate([near_f, near_b], axis=1).astype(BF16), states,
            preferred_element_type=F32,
        )
        for h, m in enumerate(masks):
            o = o + jnp.where(m, inside[h * BLOCK : (h + 1) * BLOCK], 0.0)
        o_s[rows] = o - averaged(o, average)
        far_f = wide * jnp.exp(ldf * (l + (i * BLOCK + 1.0)))
        far_b = wide * jnp.exp(ldb * ((tokens - i * BLOCK) - l))
        readers[rows] = jnp.concatenate([far_f, far_b], axis=1).astype(BF16)

    for i in range(blocks // 2):
        near(i)
    one.wait(r1)
    got = [r1[j].astype(F32) for j in range(ny)]
    hf, hb = jnp.exp(ldf * tokens), jnp.exp(ldb * tokens)
    ahead = [jnp.zeros_like(got[0][:part])]
    for j in range(ny):
        ahead.append(hf * ahead[-1] + got[j][:part])
    total_f = ahead.pop()
    behind = [jnp.zeros_like(ahead[0])]
    for j in reversed(range(ny)):
        behind.append(hb * behind[-1] + got[j][part : 2 * part])
    total_b = behind.pop()
    behind = behind[::-1]
    ctx = sum(got)
    ctx_f, ctx_b = ctx[2 * part : 3 * part], ctx[3 * part :]
    span = float(tokens * ny)
    for k in range(nz):
        there = lax.rem(z + k, nz)
        ahead_by = (there - z).astype(F32)
        to_f = jnp.where(there > z, 1.0, 0.0) * jnp.exp(ldf * (span * jnp.maximum(ahead_by - 1.0, 0.0)))
        to_b = jnp.where(there < z, 1.0, 0.0) * jnp.exp(ldb * (span * jnp.maximum(-ahead_by - 1.0, 0.0)))
        start_f = jnp.exp(ldf * (span * there.astype(F32)))
        start_b = jnp.exp(ldb * (span * (nz - 1 - there).astype(F32)))
        s2[there] = jnp.concatenate(
            [to_f * total_f + start_f * ctx_f, to_b * total_b + start_b * ctx_b], axis=0
        ).astype(BF16)
    two = Line(at, "sp_0", nz, b_send, b_recv)
    two.start(lambda there: s2.at[there], r2)
    r2[z] = s2[z]
    for i in range(blocks // 2, blocks):
        near(i)
    wc.wait(w_yz)
    two.wait(r2)
    entering = sum(r2[j].astype(F32) for j in range(nz))
    for j in range(ny):
        s3[j] = jnp.concatenate(
            [
                ahead[j] + jnp.exp(ldf * float(tokens * j)) * entering[:part],
                behind[j] + jnp.exp(ldb * float(tokens * (ny - 1 - j))) * entering[part:],
            ],
            axis=0,
        ).astype(BF16)
    three = Line(at, "sp_1", ny, c_send, c_recv)
    three.start(lambda there: s3.at[there], ent)
    ent[y] = s3[y]
    wd.wait(w_zy)
    for a in range(nz):
        for b in range(ny):
            first = (a * ny + b) * wrows
            wall[core, first : first + wrows, 0:128] = w_yz[a, b]
            wall[core, first : first + wrows, 128:256] = w_zy[b, a]
    over = {"tp_1": 1 - core}
    w_over = remote(wall.at[core], wall.at[core], x_send.at[0], x_recv.at[0], over)
    w_over.start()
    three.wait(ent)

    slices = [ent[s].astype(F32) for s in range(ny)]
    packed = jnp.concatenate([e[:part] for e in slices] + [e[part:] for e in slices], axis=0)
    packed = packed - averaged(packed, average)
    states = jnp.concatenate(
        [spread_out(packed[:HEAD], masks), spread_out(packed[HEAD:], masks)], axis=0
    ).astype(BF16)
    order = (2, 1, 3, 0)
    right, left = lax.rem(x + 1, nx), lax.rem(x + nx - 1, nx)
    to_right, to_left = {"tp_0": right}, {"tp_0": left}
    partner = t + 1 - 2 * core
    posted = []

    def post(src, dst, q, s, r, device):
        copy = remote(src, dst, g_send.at[q, s], g_recv.at[q, r], device)
        copy.start()
        posted.append(copy)

    def arrived(q, s, r):
        remote(
            gathered.at[q, s], gathered.at[q, s], g_send.at[q, 0], g_recv.at[q, r], over
        ).wait_recv()

    for steps in order:
        q = lax.rem(x + steps, nx)
        rows = pl.ds(pl.multiple_of(q * 2 * own, 2 * own), 2 * own)
        centred = o_s[rows] + jnp.dot(readers[rows], states, preferred_element_type=F32)
        spread = averaged(centred * centred, average)
        kept = (centred * lax.rsqrt(spread + EPSILON) * hg_ref[...]).astype(BF16)
        ret[2 * q] = kept[:own]
        ret[2 * q + 1] = kept[own:]
        post(ret.at[2 * q + 1 - core], gathered.at[q, t], q, 0, 0, over)
        post(ret.at[2 * q + core], gathered.at[q, t], q, 1, 1 + core, to_right)
        post(ret.at[2 * q + core], gathered.at[q, t], q, 2, 3 + core, to_left)
        gathered[q, t] = ret[2 * q + core]
    for steps in order:
        q = lax.rem(x + steps, nx)
        arrived(q, partner, 0)
        post(gathered.at[q, partner], gathered.at[q, partner], q, 3, 2 - core, to_right)
        post(gathered.at[q, partner], gathered.at[q, partner], q, 4, 4 - core, to_left)
    for steps in order:
        q = lax.rem(left + steps, nx)
        arrived(q, 2 * left, 1)
        post(gathered.at[q, 2 * left], gathered.at[q, 2 * left], q, 5, 5, to_right)
        q = lax.rem(right + steps, nx)
        arrived(q, 2 * right + 1, 4)
        post(gathered.at[q, 2 * right + 1], gathered.at[q, 2 * right + 1], q, 6, 6, to_left)
    w_over.wait_recv()
    far = lax.rem(x + 2, nx)

    def mixed_for(qs):
        for q in qs:
            arrived(q, 2 * left + 1, 2)
            arrived(q, 2 * right, 3)
            arrived(q, 2 * far, 5)
            arrived(q, 2 * far + 1, 6)
        rows = jnp.concatenate(
            [jnp.concatenate([gathered[q, s] for s in range(nt)], axis=1) for q in qs], axis=0
        )
        for k in range(2):
            columns = pl.ds(pl.multiple_of((2 * x + k) * width, width), width)
            mixed = jnp.dot(rows, wall[k], preferred_element_type=F32)
            for i, q in enumerate(qs):
                mine = pl.ds(pl.multiple_of((2 * q + core) * own, own), own)
                result = rows_all[mine, columns].astype(F32) + mod[2:3, columns] * mixed[
                    i * own : (i + 1) * own
                ]
                done[q, :, k * width : (k + 1) * width] = result.astype(BF16)

    def give(steps):
        q = lax.rem(x + steps, nx)
        copy = remote(done.at[q], landed.at[x], o_send.at[steps], o_recv.at[x], {"tp_0": q})
        copy.start()
        posted.append(copy)

    mixed_for([far])
    give(2)
    mixed_for([right, left])
    give(1)
    give(nx - 1)
    mixed_for([x])
    landed[x] = done[x]
    for chip in (right, left, far):
        remote(
            landed.at[chip], landed.at[chip], o_send.at[0], o_recv.at[chip], {"tp_0": chip}
        ).wait_recv()
    for chip in range(nx):
        out_ref[:, chip * 2 * width : (chip + 1) * 2 * width] = landed[chip]
    for line in (along_y, along_z, wa, wb, wc, wd, one, two, three, spread_rows):
        line.drain()
    for copy in sent + posted + [w_over]:
        copy.wait_send()


def turns(positions):
    frequency = ROTARY_BASE ** -np.linspace(0.0, 1.0, HALF)
    angles = np.asarray(positions, np.float64)[:, None] * frequency[None]
    tile = lambda a: np.tile(np.asarray(a, np.float32), (1, 128 // HALF))
    return tile(np.cos(angles)), tile(np.sin(angles))


def per_device(
    sizes, latent, context, condition, context_condition, modulation_weight, norm_gain,
    query_weight, key_weight, value_weight, log_decay, head_gain, output_weight,
):
    ny, nz, nx = sizes
    nt = 2 * nx
    d = latent.shape[1]
    width = query_weight.shape[1]
    heads = width // HEAD
    own = latent.shape[0]
    tokens = own * nt
    ctx_rows = context.shape[0]
    ctx_len = ctx_rows * ny * nz
    wrows = output_weight.shape[0]
    cos_off, sin_off = turns(np.arange(tokens))
    bases = np.stack(
        turns(ctx_len + tokens * np.arange(ny * nz)) + turns(ctx_rows * np.arange(ny * nz)), axis=1
    )
    ins = [
        condition.reshape(1, d), context_condition.reshape(1, d),
        modulation_weight.transpose(1, 0, 2), latent, context, output_weight, norm_gain.reshape(1, d),
        log_decay, head_gain.reshape(1, width), jnp.asarray(cos_off), jnp.asarray(sin_off),
        jnp.asarray(bases), query_weight, key_weight, value_weight,
    ]
    dma = lambda *n: pltpu.SemaphoreType.DMA(n)
    part, blocks = HEAD // ny, tokens // BLOCK
    pair = lambda n: [dma(n), dma(n)]
    scratch = [
        pltpu.VMEM(shape, kind)
        for shape, kind in (
            *[((d, width), BF16)] * 3,
            ((8, width), F32), ((8, d), F32), ((tokens, d), BF16), ((tokens, 128), F32),
            ((tokens + ctx_rows, d), BF16), ((tokens, width), F32), ((tokens, width), F32),
            ((heads * BLOCK, BLOCK), F32),
            ((ny, 8, width), F32), ((nz, 8, width), F32), ((nt, 8, width), F32),
            ((8, width), F32), ((8, width), F32),
            ((nz, ny, wrows, 128), BF16), ((ny, nz, wrows, 128), BF16), ((2, d, width), BF16),
            ((tokens + ctx_rows, width), F32), ((tokens + ctx_rows, width), F32),
            ((tokens, width), BF16), ((tokens, width), BF16), ((tokens, width), BF16),
            ((2 * blocks, HEAD, width), F32),
            ((tokens, width), F32), ((tokens, 2 * width), BF16),
            ((ny, 4 * part, width), BF16), ((ny, 4 * part, width), BF16),
            ((nz, 2 * part, width), BF16), ((nz, 2 * part, width), BF16),
            ((ny, 2 * part, width), BF16), ((ny, 2 * part, width), BF16),
            ((nt, own, width), BF16), ((nx, nt, own, width), BF16),
            ((nx, own, 2 * width), BF16), ((nx, own, 2 * width), BF16),
        )
    ] + [
        dma(3), *pair(ny), *pair(nz), *pair(nt), *pair(GATHER_SEMS),
        *pair(ny), *pair(nz), *pair(nz), *pair(ny),
        *pair(ny), *pair(nz), *pair(ny), dma(nx, 7), dma(nx, 7), *pair(nx), *pair(1),
    ]
    near = pl.BlockSpec(memory_space=pltpu.VMEM)
    return pl.pallas_call(
        functools.partial(whole_kernel, sizes, ctx_len),
        out_shape=jax.ShapeDtypeStruct((own, d), BF16),
        in_specs=[near] * (len(ins) - 3) + [pl.BlockSpec(memory_space=pl.ANY)] * 3,
        out_specs=near,
        scratch_shapes=scratch,
        compiler_params=pltpu.CompilerParams(
            vmem_limit_bytes=VMEM_LIMIT, collective_id=0, has_side_effects=True
        ),
    )(*ins)


def solution(mesh, ny=8, nz=8, nx=4):
    split = Mesh(mesh.devices.reshape(nz, ny, nx, 2), SP_TP)
    placed = (
        P(SP_TP, None), P(SP, None), P(), P(), P(SP, None, TP), P(), P(None, TP), P(None, TP),
        P(None, TP), P(None, TP), P(TP), P(SP, None),
    )
    return jax.shard_map(
        functools.partial(per_device, (ny, nz, nx)), mesh=split, in_specs=placed,
        out_specs=P(SP_TP, None), check_vma=False,
    )
```

```python
import functools

import jax
import jax.numpy as jnp
import numpy as np
from jax import lax
from jax.experimental import pallas as pl
from jax.experimental.pallas import tpu as pltpu
from jax.sharding import Mesh
from jax.sharding import PartitionSpec as P

HEAD = 64
HALF = HEAD // 2
BLOCK = 128
SP = ("sp_0", "sp_1")
TP = ("tp_0", "tp_1")
SP_TP = SP + TP
EPSILON = 1e-06
ROTARY_BASE = 10000.0
F32, BF16 = jnp.float32, jnp.bfloat16
MESH = pl.DeviceIdType.MESH
VMEM_LIMIT = 60 * 1024 * 1024


def remote(src, dst, send_sem, recv_sem, device):
    return pltpu.make_async_remote_copy(
        src_ref=src, dst_ref=dst, send_sem=send_sem, recv_sem=recv_sem,
        device_id=device, device_id_type=MESH,
    )


def place():
    return {a: lax.axis_index(a) for a in SP_TP}


def tp_peers(at, nx):
    core, x = at["tp_1"], at["tp_0"]
    peers = []
    for k in sorted(range(1, nx), key=lambda k: -min(k, nx - k)):
        peers.append({"tp_0": lax.rem(x + k, nx), "tp_1": 1 - core})
    peers.append({"tp_0": x, "tp_1": 1 - core})
    for k in sorted(range(1, nx), key=lambda k: -min(k, nx - k)):
        peers.append({"tp_0": lax.rem(x + k, nx), "tp_1": core})
    return peers


def line_peers(at, axis, n):
    return [{axis: lax.rem(at[axis] + k, n)} for k in range(1, n)]


def greet(peers):
    barrier = pltpu.get_barrier_semaphore()
    for peer in peers:
        pl.semaphore_signal(barrier, inc=1, device_id=peer, device_id_type=MESH)
    return lambda: pl.semaphore_wait(barrier, len(peers))


class Line:
    def __init__(self, at, axis, n, send_sems, recv_sems):
        self.me, self.axis, self.n = at[axis], axis, n
        self.send_sems, self.recv_sems = send_sems, recv_sems
        self.sent = []

    def start(self, source_of, slots):
        for k in sorted(range(1, self.n), key=lambda k: -min(k, self.n - k)):
            there = lax.rem(self.me + k, self.n)
            copy = remote(
                source_of(there), slots.at[self.me], self.send_sems.at[k],
                self.recv_sems.at[self.me], {self.axis: there},
            )
            copy.start()
            self.sent.append(copy)

    def wait(self, slots):
        for k in range(1, self.n):
            source = lax.rem(self.me + self.n - k, self.n)
            remote(
                slots.at[source], slots.at[source], self.send_sems.at[k],
                self.recv_sems.at[source], {self.axis: source},
            ).wait_recv()

    def drain(self):
        for copy in self.sent:
            copy.wait_send()


class Gather:
    def __init__(self, at, nx, rows, slot, sems):
        self.x, self.core, self.nx, self.rows, self.slot = at["tp_0"], at["tp_1"], nx, rows, slot
        self.send_sems, self.recv_sems = sems
        self.half = rows // 2
        self.sent = []

    def index(self, steps):
        return lax.rem(self.x + self.nx + steps, self.nx)

    def put(self, src, x_of, core_of, first, count, sem, device):
        copy = remote(
            src, self.slot(x_of * 2 + core_of, first, count), self.send_sems.at[sem],
            self.recv_sems.at[sem], device,
        )
        copy.start()
        self.sent.append(copy)

    def came(self, x_of, core_of, first, count, sem):
        view = self.slot(x_of * 2 + core_of, first, count)
        remote(view, view, self.send_sems.at[sem], self.recv_sems.at[sem], {"tp_0": self.x}).wait_recv()

    def start(self, own):
        x, core, h = self.x, self.core, self.half
        right, left = {"tp_0": self.index(1)}, {"tp_0": self.index(-1)}
        self.put(own(0, h), x, core, 0, h, 0, right)
        self.put(own(h, h), x, core, h, h, 2, left)
        self.put(own(h, h), x, core, h, h, 1, right)
        self.put(own(0, h), x, core, 0, h, 3, left)
        self.put(own(0, self.rows), x, core, 0, self.rows, 6, {"tp_1": 1 - core})

    def forward(self):
        core, h = self.core, self.half
        left, right, over = self.index(-1), self.index(1), {"tp_1": 1 - core}
        self.came(left, core, 0, h, 0)
        self.put(self.slot(left * 2 + core, 0, h), left, core, 0, h, 4, {"tp_0": right})
        self.came(right, core, h, h, 2)
        self.put(self.slot(right * 2 + core, h, h), right, core, h, h, 5, {"tp_0": left})
        self.came(left, core, h, h, 1)
        self.put(self.slot(left * 2 + core, 0, self.rows), left, core, 0, self.rows, 7, over)
        self.came(right, core, 0, h, 3)
        self.put(self.slot(right * 2 + core, 0, self.rows), right, core, 0, self.rows, 8, over)

    def finish(self):
        core, h, n = self.core, self.half, self.rows
        far, over = self.index(2), {"tp_1": 1 - core}
        self.came(far, core, 0, h, 4)
        self.came(far, core, h, h, 5)
        self.put(self.slot(far * 2 + core, 0, n), far, core, 0, n, 9, over)
        for sem, steps in ((6, 0), (7, -1), (8, 1), (9, 2)):
            self.came(self.index(steps), 1 - core, 0, n, sem)

    def drain(self):
        for copy in self.sent:
            copy.wait_send()


GATHER_SEMS = 10


def head_masks(heads):
    lane = lax.broadcasted_iota(jnp.int32, (1, heads * HEAD), 1)
    return [(lane >= h * HEAD) & (lane < (h + 1) * HEAD) for h in range(heads)]


def squeezed(full, masks):
    return sum(
        jnp.where(m, full[h * HEAD : (h + 1) * HEAD], 0.0) for h, m in enumerate(masks)
    )


def spread_out(packed, masks):
    return jnp.concatenate([jnp.where(m, packed, 0.0) for m in masks], axis=0)


def rotated(u, cos, sin, low):
    width = u.shape[1]
    partner = jnp.where(low, pltpu.roll(u, width - HALF, 1), pltpu.roll(u, HALF, 1))
    return u * cos + partner * sin


def outer(keys, values):
    return lax.dot_general(
        keys.astype(BF16), values, (((0,), (0,)), ((), ())), preferred_element_type=F32
    )


def averaged(values, average):
    high = values.astype(BF16)
    rest = (values - high.astype(F32)).astype(BF16)
    return jnp.dot(high, average, preferred_element_type=F32) + jnp.dot(
        rest, average, preferred_element_type=F32
    )


def whole_kernel(
    sizes, ctx_len, cond_ref, other_ref, mw_ref, lat_ref, ctx_ref, w_ref, gain_ref, ld_ref, hg_ref,
    cos_hbm, sin_hbm, base_hbm, wq_hbm, wk_hbm, wv_hbm, out_ref,
    cos_ref, sin_ref, base_ref, wq, wk, wv, part_s, mod, rows_all, stat, normed, cos_s, sin_s, decay,
    ybuf, zbuf, tbuf, ysum, zsum, w_yz, w_zy, wall,
    k_sum, v_sum, k_s, v_s, q_s, u_s, o_s, readers, st, r1, s2, r2, s3, ent, ret, gathered, done, landed,
    wt_sem, y_send, y_recv, z_send, z_recv, t_send, t_recv, l_send, l_recv,
    wa_send, wa_recv, wb_send, wb_recv, wc_send, wc_recv, wd_send, wd_recv,
    a_send, a_recv, b_send, b_recv, c_send, c_recv, g_send, g_recv, o_send, o_recv, x_send, x_recv,
):
    ny, nz, nx = sizes
    nt = 2 * nx
    own, d = lat_ref.shape
    tokens = own * nt
    width = hg_ref.shape[1]
    heads = width // HEAD
    blocks = tokens // BLOCK
    part = HEAD // ny
    ctx_rows = ctx_ref.shape[0]
    at = place()
    y, z, x, core = at["sp_1"], at["sp_0"], at["tp_0"], at["tp_1"]
    t, sp = x * 2 + core, z * ny + y
    tps = tp_peers(at, nx)
    met = greet(line_peers(at, "sp_1", ny) + line_peers(at, "sp_0", nz) + tps)
    fetched = (
        (wk_hbm, wk), (wv_hbm, wv), (wq_hbm, wq),
        (cos_hbm, cos_ref), (sin_hbm, sin_ref), (base_hbm.at[sp], base_ref),
    )
    weights = [
        pltpu.make_async_copy(a, b, wt_sem.at[i]) for i, (a, b) in enumerate(fetched)
    ]
    for copy in weights[3:] + weights[:3]:
        copy.start()

    c = jnp.concatenate([cond_ref[...], other_ref[...], jnp.zeros((6, d), F32)], axis=0)
    activated = (c / (1.0 + jnp.exp(-c))).astype(BF16)
    _, depth, cols = mw_ref.shape
    entry = lax.broadcasted_iota(jnp.int32, (d, depth), 0)
    place_of = lax.broadcasted_iota(jnp.int32, (d, depth), 1) + sp * depth
    mine = jnp.dot(
        activated, jnp.where(entry == place_of, 1.0, 0.0).astype(BF16), preferred_element_type=F32
    ).astype(BF16)
    parts = [jnp.dot(mine, mw_ref[r], preferred_element_type=F32) for r in range(3)]
    part_s[...] = jnp.concatenate(
        [parts[r][k : k + 1] for k in range(2) for r in range(3)] + [parts[0][2:4]], axis=0
    )
    met()
    along_y = Line(at, "sp_1", ny, y_send, y_recv)
    along_z = Line(at, "sp_0", nz, z_send, z_recv)
    along_y.start(lambda there: part_s, ybuf)
    spread_rows = Gather(
        at, nx, own, lambda s, a, n: rows_all.at[pl.ds(s * own + a, n)], (l_send, l_recv)
    )
    spread_rows.start(lambda a, n: lat_ref.at[pl.ds(a, n)])
    ybuf[y] = part_s[...]
    rows_all[pl.ds(pl.multiple_of(t * own, own), own)] = lat_ref[...]
    wrows = w_ref.shape[0]
    w_yz[z, y] = w_ref[:, pl.ds(pl.multiple_of(t * 256, 256), 128)]
    w_zy[y, z] = w_ref[:, pl.ds(pl.multiple_of(t * 256 + 128, 128), 128)]
    wa = Line(at, "sp_1", ny, wa_send, wa_recv)
    wa.start(lambda there: w_yz.at[z, y], w_yz.at[z])
    wb = Line(at, "sp_0", nz, wb_send, wb_recv)
    wb.start(lambda there: w_zy.at[y, z], w_zy.at[y])

    lane = lax.broadcasted_iota(jnp.int32, (1, width), 1)
    low = lax.rem(lane, HEAD) < HALF
    sign = jnp.where(low, -1.0, 1.0)
    repeat = lambda a: jnp.concatenate([a] * (width // a.shape[1]), axis=1)
    for copy in weights[3:]:
        copy.wait()
    base = repeat(base_ref[...])
    cos_off, sin_off = repeat(cos_ref[...]), repeat(sin_ref[...])
    cos_s[...] = base[0:1] * cos_off - base[1:2] * sin_off
    sin_s[...] = (base[1:2] * cos_off + base[0:1] * sin_off) * sign
    ccos = base[2:3] * cos_off[:ctx_rows] - base[3:4] * sin_off[:ctx_rows]
    csin = (base[3:4] * cos_off[:ctx_rows] + base[2:3] * sin_off[:ctx_rows]) * sign
    masks = head_masks(heads)
    rates = sum(jnp.where(m, ld_ref[:, h : h + 1], 0.0) for h, m in enumerate(masks))
    ldf, ldb = rates[0:1], rates[1:2]
    row = lax.broadcasted_iota(jnp.int32, (BLOCK, BLOCK), 0)
    col = lax.broadcasted_iota(jnp.int32, (BLOCK, BLOCK), 1)
    gap = (row - col).astype(F32)
    for h in range(heads):
        f, b = ldf[:, h * HEAD : h * HEAD + 1], ldb[:, h * HEAD : h * HEAD + 1]
        decay[h * BLOCK : (h + 1) * BLOCK] = jnp.where(
            gap >= 0, jnp.exp(f * jnp.maximum(gap, 0.0)), 0.0
        ) + jnp.where(gap <= 0, jnp.exp(b * jnp.maximum(-gap, 0.0)), 0.0)

    along_y.wait(ybuf)
    ysum[...] = sum(ybuf[k] for k in range(ny))
    along_z.start(lambda there: ysum, zbuf)
    zbuf[z] = ysum[...]
    wb.wait(w_zy.at[y])
    wd = Line(at, "sp_1", ny, wd_send, wd_recv)
    wd.start(lambda there: w_zy.at[y], w_zy)
    spread_rows.forward()
    along_z.wait(zbuf)
    zsum[...] = sum(zbuf[k] for k in range(nz))
    sent = []
    for k, peer in enumerate(tps):
        copy = remote(zsum, tbuf.at[t], t_send.at[k], t_recv.at[t], peer)
        copy.start()
        sent.append(copy)
    tbuf[t] = zsum[...]
    wa.wait(w_yz.at[z])
    wc = Line(at, "sp_0", nz, wc_send, wc_recv)
    wc.start(lambda there: w_yz.at[z], w_yz)
    spread_rows.finish()

    def root(rows):
        wide = rows.astype(F32)
        return lax.rsqrt(jnp.mean(wide * wide, axis=-1, keepdims=True) + EPSILON)

    @pl.loop(0, tokens // 64)
    def _(i):
        rows = pl.ds(pl.multiple_of(i * 64, 64), 64)
        stat[rows] = jnp.broadcast_to(root(rows_all[rows]), (64, 128))

    ctx_root = root(ctx_ref[...])

    def came(s):
        remote(
            tbuf.at[s], tbuf.at[s], t_send.at[0], t_recv.at[s], {"tp_1": 1 - core}
        ).wait_recv()

    def norm(rows, r, k, columns):
        scale = gain_ref[:, columns] * (1.0 + mod[3 * k + 1 : 3 * k + 2, columns])
        return (rows.astype(F32) * r * scale + mod[3 * k : 3 * k + 1, columns]).astype(BF16)

    for steps in (0, 1, 3, 2):
        chip = lax.rem(x + steps, nx)
        came(2 * chip + 1 - core)
        if steps:
            came(2 * chip + core)
        for k in range(2):
            columns = pl.ds(pl.multiple_of(chip * 512 + k * 256, 256), 256)
            mod[:, columns] = tbuf[2 * chip + k]
        if steps == 0:
            weights[0].wait()
            weights[1].wait()
        for k in range(2):
            columns = pl.ds(pl.multiple_of(chip * 512 + k * 256, 256), 256)
            r = jnp.concatenate([stat[...]] * 2, axis=1)
            normed[0:tokens, columns] = norm(rows_all[:, columns], r, 0, columns)
            normed[tokens : tokens + ctx_rows, columns] = norm(
                ctx_ref[:, columns], ctx_root, 1, columns
            )
        columns = pl.ds(pl.multiple_of(chip * 512, 512), 512)
        k_more = jnp.dot(normed[:, columns], wk[columns], preferred_element_type=F32)
        v_more = jnp.dot(normed[:, columns], wv[columns], preferred_element_type=F32)
        if steps == 0:
            k_sum[...] = k_more
            v_sum[...] = v_more
        elif steps != 2:
            k_sum[...] += k_more
            v_sum[...] += v_more
        else:
            k_all = k_sum[...] + k_more
            v_all = (v_sum[...] + v_more).astype(BF16)
    v_s[...] = v_all[:tokens]
    k_s[...] = rotated(k_all[:tokens], cos_s[...], sin_s[...], low).astype(BF16)
    ck = rotated(k_all[tokens:], ccos, csin, low).astype(BF16).astype(F32)
    cv = v_all[tokens:]
    spot = (sp * ctx_rows + lax.broadcasted_iota(jnp.int32, (ctx_rows, 1), 0)).astype(F32)
    cf = squeezed(outer(ck * jnp.exp(ldf * (ctx_len - 1.0 - spot)), cv), masks)
    cb = squeezed(outer(ck * jnp.exp(ldb * spot), cv), masks)
    l = lax.broadcasted_iota(jnp.int32, (BLOCK, 1), 0).astype(F32)
    to_end, to_start = jnp.exp(ldf * (BLOCK - 1.0 - l)), jnp.exp(ldb * l)
    gf, gb = jnp.exp(ldf * BLOCK), jnp.exp(ldb * BLOCK)
    sf = jnp.zeros((HEAD, width), F32)
    ub = []
    for b in range(blocks):
        keys = k_s[b * BLOCK : (b + 1) * BLOCK].astype(F32)
        values = v_s[b * BLOCK : (b + 1) * BLOCK]
        u_s[b] = sf
        sf = gf * sf + squeezed(outer(keys * to_end, values), masks)
        ub.append(squeezed(outer(keys * to_start, values), masks))
    sb = jnp.zeros((HEAD, width), F32)
    for b in reversed(range(blocks)):
        u_s[blocks + b] = sb
        sb = gb * sb + ub[b]
    for s in range(ny):
        rows = slice(s * part, (s + 1) * part)
        st[s] = jnp.concatenate([sf[rows], sb[rows], cf[rows], cb[rows]], axis=0).astype(BF16)
    one = Line(at, "sp_1", ny, a_send, a_recv)
    one.start(lambda there: st.at[there], r1)
    r1[y] = st[y]

    weights[2].wait()
    q_all = jnp.dot(normed[0:tokens], wq[...], preferred_element_type=F32)
    queries = (rotated(q_all, cos_s[...], sin_s[...], low) * HEAD ** (-0.5)).astype(BF16)
    read_f, read_b = jnp.exp(ldf * (l + 1.0)), jnp.exp(ldb * (BLOCK - l))
    a = lax.broadcasted_iota(jnp.int32, (width, width), 0)
    b = lax.broadcasted_iota(jnp.int32, (width, width), 1)
    average = jnp.where(a // HEAD == b // HEAD, 1.0 / HEAD, 0.0).astype(BF16)
    q_s[...] = queries

    def near(i):
        rows = slice(i * BLOCK, (i + 1) * BLOCK)
        wide = q_s[rows].astype(F32)
        stacked = jnp.concatenate([jnp.where(m, wide, 0.0) for m in masks], axis=0).astype(BF16)
        scores = lax.dot_general(
            stacked, k_s[rows], (((1,), (1,)), ((), ())), preferred_element_type=F32
        )
        inside = jnp.dot(
            (scores * decay[...]).astype(BF16), v_s[rows], preferred_element_type=F32
        )
        states = jnp.concatenate(
            [spread_out(u_s[i], masks), spread_out(u_s[blocks + i], masks)], axis=0
        ).astype(BF16)
        near_f, near_b = wide * read_f, wide * read_b
        o = jnp.dot(
            jnp.concatenate([near_f, near_b], axis=1).astype(BF16), states,
            preferred_element_type=F32,
        )
        for h, m in enumerate(masks):
            o = o + jnp.where(m, inside[h * BLOCK : (h + 1) * BLOCK], 0.0)
        o_s[rows] = o - averaged(o, average)
        far_f = wide * jnp.exp(ldf * (l + (i * BLOCK + 1.0)))
        far_b = wide * jnp.exp(ldb * ((tokens - i * BLOCK) - l))
        readers[rows] = jnp.concatenate([far_f, far_b], axis=1).astype(BF16)

    for i in range(blocks // 2):
        near(i)
    span = float(tokens * ny)
    factors = []
    for k in range(nz):
        there = lax.rem(z + k, nz)
        ahead_by = (there - z).astype(F32)
        to_f = jnp.where(there > z, 1.0, 0.0) * jnp.exp(ldf * (span * jnp.maximum(ahead_by - 1.0, 0.0)))
        to_b = jnp.where(there < z, 1.0, 0.0) * jnp.exp(ldb * (span * jnp.maximum(-ahead_by - 1.0, 0.0)))
        start_f = jnp.exp(ldf * (span * there.astype(F32)))
        start_b = jnp.exp(ldb * (span * (nz - 1 - there).astype(F32)))
        factors.append((there, to_f, to_b, start_f, start_b))
    one.wait(r1)
    got = [r1[j].astype(F32) for j in range(ny)]
    hf, hb = jnp.exp(ldf * tokens), jnp.exp(ldb * tokens)
    ahead = [jnp.zeros_like(got[0][:part])]
    for j in range(ny):
        ahead.append(hf * ahead[-1] + got[j][:part])
    total_f = ahead.pop()
    behind = [jnp.zeros_like(ahead[0])]
    for j in reversed(range(ny)):
        behind.append(hb * behind[-1] + got[j][part : 2 * part])
    total_b = behind.pop()
    behind = behind[::-1]
    ctx = sum(got)
    ctx_f, ctx_b = ctx[2 * part : 3 * part], ctx[3 * part :]
    for there, to_f, to_b, start_f, start_b in factors:
        s2[there] = jnp.concatenate(
            [to_f * total_f + start_f * ctx_f, to_b * total_b + start_b * ctx_b], axis=0
        ).astype(BF16)
    two = Line(at, "sp_0", nz, b_send, b_recv)
    two.start(lambda there: s2.at[there], r2)
    r2[z] = s2[z]
    for i in range(blocks // 2, blocks):
        near(i)
    wc.wait(w_yz)
    two.wait(r2)
    entering = sum(r2[j].astype(F32) for j in range(nz))
    for j in range(ny):
        s3[j] = jnp.concatenate(
            [
                ahead[j] + jnp.exp(ldf * float(tokens * j)) * entering[:part],
                behind[j] + jnp.exp(ldb * float(tokens * (ny - 1 - j))) * entering[part:],
            ],
            axis=0,
        ).astype(BF16)
    three = Line(at, "sp_1", ny, c_send, c_recv)
    three.start(lambda there: s3.at[there], ent)
    ent[y] = s3[y]
    wd.wait(w_zy)
    for a in range(nz):
        for b in range(ny):
            first = (a * ny + b) * wrows
            wall[core, first : first + wrows, 0:128] = w_yz[a, b]
            wall[core, first : first + wrows, 128:256] = w_zy[b, a]
    over = {"tp_1": 1 - core}
    w_over = remote(wall.at[core], wall.at[core], x_send.at[0], x_recv.at[0], over)
    w_over.start()
    three.wait(ent)

    slices = [ent[s].astype(F32) for s in range(ny)]
    packed = jnp.concatenate([e[:part] for e in slices] + [e[part:] for e in slices], axis=0)
    packed = packed - averaged(packed, average)
    states = jnp.concatenate(
        [spread_out(packed[:HEAD], masks), spread_out(packed[HEAD:], masks)], axis=0
    ).astype(BF16)
    order = (2, 1, 3, 0)
    right, left = lax.rem(x + 1, nx), lax.rem(x + nx - 1, nx)
    to_right, to_left = {"tp_0": right}, {"tp_0": left}
    partner = t + 1 - 2 * core
    posted = []

    def post(src, dst, q, s, r, device):
        copy = remote(src, dst, g_send.at[q, s], g_recv.at[q, r], device)
        copy.start()
        posted.append(copy)

    def arrived(q, s, r):
        remote(
            gathered.at[q, s], gathered.at[q, s], g_send.at[q, 0], g_recv.at[q, r], over
        ).wait_recv()

    for steps in order:
        q = lax.rem(x + steps, nx)
        rows = pl.ds(pl.multiple_of(q * 2 * own, 2 * own), 2 * own)
        centred = o_s[rows] + jnp.dot(readers[rows], states, preferred_element_type=F32)
        spread = averaged(centred * centred, average)
        kept = (centred * lax.rsqrt(spread + EPSILON) * hg_ref[...]).astype(BF16)
        ret[2 * q] = kept[:own]
        ret[2 * q + 1] = kept[own:]
        post(ret.at[2 * q + 1 - core], gathered.at[q, t], q, 0, 0, over)
        post(ret.at[2 * q + core], gathered.at[q, t], q, 1, 1 + core, to_right)
        post(ret.at[2 * q + core], gathered.at[q, t], q, 2, 3 + core, to_left)
        gathered[q, t] = ret[2 * q + core]
    for steps in order:
        q = lax.rem(x + steps, nx)
        arrived(q, partner, 0)
        post(gathered.at[q, partner], gathered.at[q, partner], q, 3, 2 - core, to_right)
        post(gathered.at[q, partner], gathered.at[q, partner], q, 4, 4 - core, to_left)
    for steps in order:
        q = lax.rem(left + steps, nx)
        arrived(q, 2 * left, 1)
        post(gathered.at[q, 2 * left], gathered.at[q, 2 * left], q, 5, 5, to_right)
        q = lax.rem(right + steps, nx)
        arrived(q, 2 * right + 1, 4)
        post(gathered.at[q, 2 * right + 1], gathered.at[q, 2 * right + 1], q, 6, 6, to_left)
    w_over.wait_recv()
    far = lax.rem(x + 2, nx)

    def mixed_for(qs):
        for q in qs:
            arrived(q, 2 * left + 1, 2)
            arrived(q, 2 * right, 3)
            arrived(q, 2 * far, 5)
            arrived(q, 2 * far + 1, 6)
        rows = jnp.concatenate(
            [jnp.concatenate([gathered[q, s] for s in range(nt)], axis=1) for q in qs], axis=0
        )
        for k in range(2):
            columns = pl.ds(pl.multiple_of((2 * x + k) * width, width), width)
            mixed = jnp.dot(rows, wall[k], preferred_element_type=F32)
            for i, q in enumerate(qs):
                mine = pl.ds(pl.multiple_of((2 * q + core) * own, own), own)
                result = rows_all[mine, columns].astype(F32) + mod[2:3, columns] * mixed[
                    i * own : (i + 1) * own
                ]
                done[q, :, k * width : (k + 1) * width] = result.astype(BF16)

    def give(steps):
        q = lax.rem(x + steps, nx)
        copy = remote(done.at[q], landed.at[x], o_send.at[steps], o_recv.at[x], {"tp_0": q})
        copy.start()
        posted.append(copy)

    mixed_for([far])
    give(2)
    mixed_for([right, left])
    give(1)
    give(nx - 1)
    mixed_for([x])
    landed[x] = done[x]
    for chip in (right, left, far):
        remote(
            landed.at[chip], landed.at[chip], o_send.at[0], o_recv.at[chip], {"tp_0": chip}
        ).wait_recv()
    for chip in range(nx):
        out_ref[:, chip * 2 * width : (chip + 1) * 2 * width] = landed[chip]
    for line in (along_y, along_z, wa, wb, wc, wd, one, two, three, spread_rows):
        line.drain()
    for copy in sent + posted + [w_over]:
        copy.wait_send()


def turns(positions):
    frequency = ROTARY_BASE ** -np.linspace(0.0, 1.0, HALF)
    angles = np.asarray(positions, np.float64)[:, None] * frequency[None]
    tile = lambda a: np.tile(np.asarray(a, np.float32), (1, 128 // HALF))
    return tile(np.cos(angles)), tile(np.sin(angles))


def per_device(
    sizes, latent, context, condition, context_condition, modulation_weight, norm_gain,
    query_weight, key_weight, value_weight, log_decay, head_gain, output_weight,
):
    ny, nz, nx = sizes
    nt = 2 * nx
    d = latent.shape[1]
    width = query_weight.shape[1]
    heads = width // HEAD
    own = latent.shape[0]
    tokens = own * nt
    ctx_rows = context.shape[0]
    ctx_len = ctx_rows * ny * nz
    wrows = output_weight.shape[0]
    cos_off, sin_off = turns(np.arange(tokens))
    bases = np.stack(
        turns(ctx_len + tokens * np.arange(ny * nz)) + turns(ctx_rows * np.arange(ny * nz)), axis=1
    )
    ins = [
        condition.reshape(1, d), context_condition.reshape(1, d),
        modulation_weight.transpose(1, 0, 2), latent, context, output_weight, norm_gain.reshape(1, d),
        log_decay, head_gain.reshape(1, width), jnp.asarray(cos_off), jnp.asarray(sin_off),
        jnp.asarray(bases), query_weight, key_weight, value_weight,
    ]
    dma = lambda *n: pltpu.SemaphoreType.DMA(n)
    part, blocks = HEAD // ny, tokens // BLOCK
    pair = lambda n: [dma(n), dma(n)]
    scratch = [
        pltpu.VMEM(shape, kind)
        for shape, kind in (
            ((tokens, 128), F32), ((tokens, 128), F32), ((4, 128), F32),
            *[((d, width), BF16)] * 3,
            ((8, width), F32), ((8, d), F32), ((tokens, d), BF16), ((tokens, 128), F32),
            ((tokens + ctx_rows, d), BF16), ((tokens, width), F32), ((tokens, width), F32),
            ((heads * BLOCK, BLOCK), F32),
            ((ny, 8, width), F32), ((nz, 8, width), F32), ((nt, 8, width), F32),
            ((8, width), F32), ((8, width), F32),
            ((nz, ny, wrows, 128), BF16), ((ny, nz, wrows, 128), BF16), ((2, d, width), BF16),
            ((tokens + ctx_rows, width), F32), ((tokens + ctx_rows, width), F32),
            ((tokens, width), BF16), ((tokens, width), BF16), ((tokens, width), BF16),
            ((2 * blocks, HEAD, width), F32),
            ((tokens, width), F32), ((tokens, 2 * width), BF16),
            ((ny, 4 * part, width), BF16), ((ny, 4 * part, width), BF16),
            ((nz, 2 * part, width), BF16), ((nz, 2 * part, width), BF16),
            ((ny, 2 * part, width), BF16), ((ny, 2 * part, width), BF16),
            ((nt, own, width), BF16), ((nx, nt, own, width), BF16),
            ((nx, own, 2 * width), BF16), ((nx, own, 2 * width), BF16),
        )
    ] + [
        dma(6), *pair(ny), *pair(nz), *pair(nt), *pair(GATHER_SEMS),
        *pair(ny), *pair(nz), *pair(nz), *pair(ny),
        *pair(ny), *pair(nz), *pair(ny), dma(nx, 7), dma(nx, 7), *pair(nx), *pair(1),
    ]
    near = pl.BlockSpec(memory_space=pltpu.VMEM)
    return pl.pallas_call(
        functools.partial(whole_kernel, sizes, ctx_len),
        out_shape=pltpu.VMEM((own, d), BF16),
        in_specs=[near] * (len(ins) - 6) + [pl.BlockSpec(memory_space=pl.ANY)] * 6,
        out_specs=near,
        scratch_shapes=scratch,
        compiler_params=pltpu.CompilerParams(
            vmem_limit_bytes=VMEM_LIMIT, collective_id=0, has_side_effects=True
        ),
    )(*ins)


def solution(mesh, ny=8, nz=8, nx=4):
    split = Mesh(mesh.devices.reshape(nz, ny, nx, 2), SP_TP)
    placed = (
        P(SP_TP, None), P(SP, None), P(), P(), P(SP, None, TP), P(), P(None, TP), P(None, TP),
        P(None, TP), P(None, TP), P(TP), P(SP, None),
    )
    return jax.shard_map(
        functools.partial(per_device, (ny, nz, nx)), mesh=split, in_specs=placed,
        out_specs=P(SP_TP, None), check_vma=False,
    )
```

```python
import functools

import jax
import jax.numpy as jnp
import numpy as np
from jax import lax
from jax.experimental import pallas as pl
from jax.experimental.pallas import tpu as pltpu
from jax.sharding import Mesh
from jax.sharding import PartitionSpec as P

HEAD = 64
HALF = HEAD // 2
BLOCK = 128
SP = ("sp_0", "sp_1")
TP = ("tp_0", "tp_1")
SP_TP = SP + TP
EPSILON = 1e-06
ROTARY_BASE = 10000.0
F32, BF16 = jnp.float32, jnp.bfloat16
MESH = pl.DeviceIdType.MESH
VMEM_LIMIT = 60 * 1024 * 1024


def remote(src, dst, send_sem, recv_sem, device):
    return pltpu.make_async_remote_copy(
        src_ref=src, dst_ref=dst, send_sem=send_sem, recv_sem=recv_sem,
        device_id=device, device_id_type=MESH,
    )


def place():
    return {a: lax.axis_index(a) for a in SP_TP}


def tp_peers(at, nx):
    core, x = at["tp_1"], at["tp_0"]
    peers = []
    for k in sorted(range(1, nx), key=lambda k: -min(k, nx - k)):
        peers.append({"tp_0": lax.rem(x + k, nx), "tp_1": 1 - core})
    peers.append({"tp_0": x, "tp_1": 1 - core})
    for k in sorted(range(1, nx), key=lambda k: -min(k, nx - k)):
        peers.append({"tp_0": lax.rem(x + k, nx), "tp_1": core})
    return peers


def line_peers(at, axis, n):
    return [{axis: lax.rem(at[axis] + k, n)} for k in range(1, n)]


def greet(peers):
    barrier = pltpu.get_barrier_semaphore()
    for peer in peers:
        pl.semaphore_signal(barrier, inc=1, device_id=peer, device_id_type=MESH)
    return lambda: pl.semaphore_wait(barrier, len(peers))


class Line:
    def __init__(self, at, axis, n, send_sems, recv_sems):
        self.me, self.axis, self.n = at[axis], axis, n
        self.send_sems, self.recv_sems = send_sems, recv_sems
        self.sent = []

    def start(self, source_of, slots):
        for k in sorted(range(1, self.n), key=lambda k: -min(k, self.n - k)):
            there = lax.rem(self.me + k, self.n)
            copy = remote(
                source_of(there), slots.at[self.me], self.send_sems.at[k],
                self.recv_sems.at[self.me], {self.axis: there},
            )
            copy.start()
            self.sent.append(copy)

    def wait(self, slots):
        for k in range(1, self.n):
            source = lax.rem(self.me + self.n - k, self.n)
            remote(
                slots.at[source], slots.at[source], self.send_sems.at[k],
                self.recv_sems.at[source], {self.axis: source},
            ).wait_recv()

    def drain(self):
        for copy in self.sent:
            copy.wait_send()


class Gather:
    def __init__(self, at, nx, rows, slot, sems):
        self.x, self.core, self.nx, self.rows, self.slot = at["tp_0"], at["tp_1"], nx, rows, slot
        self.send_sems, self.recv_sems = sems
        self.half = rows // 2
        self.sent = []

    def index(self, steps):
        return lax.rem(self.x + self.nx + steps, self.nx)

    def put(self, src, x_of, core_of, first, count, sem, device):
        copy = remote(
            src, self.slot(x_of * 2 + core_of, first, count), self.send_sems.at[sem],
            self.recv_sems.at[sem], device,
        )
        copy.start()
        self.sent.append(copy)

    def came(self, x_of, core_of, first, count, sem):
        view = self.slot(x_of * 2 + core_of, first, count)
        remote(view, view, self.send_sems.at[sem], self.recv_sems.at[sem], {"tp_0": self.x}).wait_recv()

    def start(self, own):
        x, core, h = self.x, self.core, self.half
        right, left = {"tp_0": self.index(1)}, {"tp_0": self.index(-1)}
        self.put(own(0, h), x, core, 0, h, 0, right)
        self.put(own(h, h), x, core, h, h, 2, left)
        self.put(own(h, h), x, core, h, h, 1, right)
        self.put(own(0, h), x, core, 0, h, 3, left)
        self.put(own(0, self.rows), x, core, 0, self.rows, 6, {"tp_1": 1 - core})

    def forward(self):
        core, h = self.core, self.half
        left, right, over = self.index(-1), self.index(1), {"tp_1": 1 - core}
        self.came(left, core, 0, h, 0)
        self.put(self.slot(left * 2 + core, 0, h), left, core, 0, h, 4, {"tp_0": right})
        self.came(right, core, h, h, 2)
        self.put(self.slot(right * 2 + core, h, h), right, core, h, h, 5, {"tp_0": left})
        self.came(left, core, h, h, 1)
        self.put(self.slot(left * 2 + core, 0, self.rows), left, core, 0, self.rows, 7, over)
        self.came(right, core, 0, h, 3)
        self.put(self.slot(right * 2 + core, 0, self.rows), right, core, 0, self.rows, 8, over)

    def finish(self):
        core, h, n = self.core, self.half, self.rows
        far, over = self.index(2), {"tp_1": 1 - core}
        self.came(far, core, 0, h, 4)
        self.came(far, core, h, h, 5)
        self.put(self.slot(far * 2 + core, 0, n), far, core, 0, n, 9, over)
        for sem, steps in ((6, 0), (7, -1), (8, 1), (9, 2)):
            self.came(self.index(steps), 1 - core, 0, n, sem)

    def drain(self):
        for copy in self.sent:
            copy.wait_send()


GATHER_SEMS = 10


def head_masks(heads):
    lane = lax.broadcasted_iota(jnp.int32, (1, heads * HEAD), 1)
    return [(lane >= h * HEAD) & (lane < (h + 1) * HEAD) for h in range(heads)]


def squeezed(full, masks):
    return sum(
        jnp.where(m, full[h * HEAD : (h + 1) * HEAD], 0.0) for h, m in enumerate(masks)
    )


def spread_out(packed, masks):
    return jnp.concatenate([jnp.where(m, packed, 0.0) for m in masks], axis=0)


def rotated(u, cos, sin, low):
    width = u.shape[1]
    partner = jnp.where(low, pltpu.roll(u, width - HALF, 1), pltpu.roll(u, HALF, 1))
    return u * cos + partner * sin


def outer(keys, values):
    return lax.dot_general(
        keys.astype(BF16), values, (((0,), (0,)), ((), ())), preferred_element_type=F32
    )


def averaged(values, average):
    high = values.astype(BF16)
    rest = (values - high.astype(F32)).astype(BF16)
    return jnp.dot(high, average, preferred_element_type=F32) + jnp.dot(
        rest, average, preferred_element_type=F32
    )


def whole_kernel(
    sizes, ctx_len, cond_ref, other_ref, mw_ref, lat_ref, ctx_ref, w_ref, gain_ref, ld_ref, hg_ref,
    cos_hbm, sin_hbm, base_hbm, wq_hbm, wk_hbm, wv_hbm, out_ref,
    cos_ref, sin_ref, base_ref, wq, wk, wv, part_s, mod, rows_all, stat, normed, cos_s, sin_s, decay,
    ybuf, zbuf, tbuf, ysum, zsum, w_yz, w_zy, wall,
    k_sum, v_sum, k_s, v_s, q_s, u_s, o_s, readers, st, r1, s2, r2, s3, ent, ret, gathered, near_sum, done, landed,
    wt_sem, y_send, y_recv, z_send, z_recv, t_send, t_recv, l_send, l_recv,
    wa_send, wa_recv, wb_send, wb_recv, wc_send, wc_recv, wd_send, wd_recv,
    a_send, a_recv, b_send, b_recv, c_send, c_recv, g_send, g_recv, o_send, o_recv, x_send, x_recv,
):
    ny, nz, nx = sizes
    nt = 2 * nx
    own, d = lat_ref.shape
    tokens = own * nt
    width = hg_ref.shape[1]
    heads = width // HEAD
    blocks = tokens // BLOCK
    part = HEAD // ny
    ctx_rows = ctx_ref.shape[0]
    at = place()
    y, z, x, core = at["sp_1"], at["sp_0"], at["tp_0"], at["tp_1"]
    t, sp = x * 2 + core, z * ny + y
    tps = tp_peers(at, nx)
    met = greet(line_peers(at, "sp_1", ny) + line_peers(at, "sp_0", nz) + tps)
    fetched = (
        (wk_hbm, wk), (wv_hbm, wv), (wq_hbm, wq),
        (cos_hbm, cos_ref), (sin_hbm, sin_ref), (base_hbm.at[sp], base_ref),
    )
    weights = [
        pltpu.make_async_copy(a, b, wt_sem.at[i]) for i, (a, b) in enumerate(fetched)
    ]
    for copy in weights[3:] + weights[:3]:
        copy.start()

    c = jnp.concatenate([cond_ref[...], other_ref[...], jnp.zeros((6, d), F32)], axis=0)
    activated = (c / (1.0 + jnp.exp(-c))).astype(BF16)
    _, depth, cols = mw_ref.shape
    entry = lax.broadcasted_iota(jnp.int32, (d, depth), 0)
    place_of = lax.broadcasted_iota(jnp.int32, (d, depth), 1) + sp * depth
    mine = jnp.dot(
        activated, jnp.where(entry == place_of, 1.0, 0.0).astype(BF16), preferred_element_type=F32
    ).astype(BF16)
    parts = [jnp.dot(mine, mw_ref[r], preferred_element_type=F32) for r in range(3)]
    part_s[...] = jnp.concatenate(
        [parts[r][k : k + 1] for k in range(2) for r in range(3)] + [parts[0][2:4]], axis=0
    )
    met()
    along_y = Line(at, "sp_1", ny, y_send, y_recv)
    along_z = Line(at, "sp_0", nz, z_send, z_recv)
    along_y.start(lambda there: part_s, ybuf)
    spread_rows = Gather(
        at, nx, own, lambda s, a, n: rows_all.at[pl.ds(s * own + a, n)], (l_send, l_recv)
    )
    spread_rows.start(lambda a, n: lat_ref.at[pl.ds(a, n)])
    ybuf[y] = part_s[...]
    rows_all[pl.ds(pl.multiple_of(t * own, own), own)] = lat_ref[...]
    wrows = w_ref.shape[0]
    w_yz[z, y] = w_ref[:, pl.ds(pl.multiple_of(t * 256, 256), 128)]
    w_zy[y, z] = w_ref[:, pl.ds(pl.multiple_of(t * 256 + 128, 128), 128)]
    wa = Line(at, "sp_1", ny, wa_send, wa_recv)
    wa.start(lambda there: w_yz.at[z, y], w_yz.at[z])
    wb = Line(at, "sp_0", nz, wb_send, wb_recv)
    wb.start(lambda there: w_zy.at[y, z], w_zy.at[y])

    lane = lax.broadcasted_iota(jnp.int32, (1, width), 1)
    low = lax.rem(lane, HEAD) < HALF
    sign = jnp.where(low, -1.0, 1.0)
    repeat = lambda a: jnp.concatenate([a] * (width // a.shape[1]), axis=1)
    for copy in weights[3:]:
        copy.wait()
    base = repeat(base_ref[...])
    cos_off, sin_off = repeat(cos_ref[...]), repeat(sin_ref[...])
    cos_s[...] = base[0:1] * cos_off - base[1:2] * sin_off
    sin_s[...] = (base[1:2] * cos_off + base[0:1] * sin_off) * sign
    ccos = base[2:3] * cos_off[:ctx_rows] - base[3:4] * sin_off[:ctx_rows]
    csin = (base[3:4] * cos_off[:ctx_rows] + base[2:3] * sin_off[:ctx_rows]) * sign
    masks = head_masks(heads)
    rates = sum(jnp.where(m, ld_ref[:, h : h + 1], 0.0) for h, m in enumerate(masks))
    ldf, ldb = rates[0:1], rates[1:2]
    row = lax.broadcasted_iota(jnp.int32, (BLOCK, BLOCK), 0)
    col = lax.broadcasted_iota(jnp.int32, (BLOCK, BLOCK), 1)
    gap = (row - col).astype(F32)
    for h in range(heads):
        f, b = ldf[:, h * HEAD : h * HEAD + 1], ldb[:, h * HEAD : h * HEAD + 1]
        decay[h * BLOCK : (h + 1) * BLOCK] = jnp.where(
            gap >= 0, jnp.exp(f * jnp.maximum(gap, 0.0)), 0.0
        ) + jnp.where(gap <= 0, jnp.exp(b * jnp.maximum(-gap, 0.0)), 0.0)

    along_y.wait(ybuf)
    ysum[...] = sum(ybuf[k] for k in range(ny))
    along_z.start(lambda there: ysum, zbuf)
    zbuf[z] = ysum[...]
    wb.wait(w_zy.at[y])
    wd = Line(at, "sp_1", ny, wd_send, wd_recv)
    wd.start(lambda there: w_zy.at[y], w_zy)
    spread_rows.forward()
    along_z.wait(zbuf)
    zsum[...] = sum(zbuf[k] for k in range(nz))
    sent = []
    for k, peer in enumerate(tps):
        copy = remote(zsum, tbuf.at[t], t_send.at[k], t_recv.at[t], peer)
        copy.start()
        sent.append(copy)
    tbuf[t] = zsum[...]
    wa.wait(w_yz.at[z])
    wc = Line(at, "sp_0", nz, wc_send, wc_recv)
    wc.start(lambda there: w_yz.at[z], w_yz)
    spread_rows.finish()

    def root(rows):
        wide = rows.astype(F32)
        return lax.rsqrt(jnp.mean(wide * wide, axis=-1, keepdims=True) + EPSILON)

    @pl.loop(0, tokens // 64)
    def _(i):
        rows = pl.ds(pl.multiple_of(i * 64, 64), 64)
        stat[rows] = jnp.broadcast_to(root(rows_all[rows]), (64, 128))

    ctx_root = root(ctx_ref[...])

    def came(s):
        remote(
            tbuf.at[s], tbuf.at[s], t_send.at[0], t_recv.at[s], {"tp_1": 1 - core}
        ).wait_recv()

    def norm(rows, r, k, columns):
        scale = gain_ref[:, columns] * (1.0 + mod[3 * k + 1 : 3 * k + 2, columns])
        return (rows.astype(F32) * r * scale + mod[3 * k : 3 * k + 1, columns]).astype(BF16)

    for steps in (0, 1, 3, 2):
        chip = lax.rem(x + steps, nx)
        came(2 * chip + 1 - core)
        if steps:
            came(2 * chip + core)
        for k in range(2):
            columns = pl.ds(pl.multiple_of(chip * 512 + k * 256, 256), 256)
            mod[:, columns] = tbuf[2 * chip + k]
        if steps == 0:
            weights[0].wait()
            weights[1].wait()
        for k in range(2):
            columns = pl.ds(pl.multiple_of(chip * 512 + k * 256, 256), 256)
            r = jnp.concatenate([stat[...]] * 2, axis=1)
            normed[0:tokens, columns] = norm(rows_all[:, columns], r, 0, columns)
            normed[tokens : tokens + ctx_rows, columns] = norm(
                ctx_ref[:, columns], ctx_root, 1, columns
            )
        columns = pl.ds(pl.multiple_of(chip * 512, 512), 512)
        k_more = jnp.dot(normed[:, columns], wk[columns], preferred_element_type=F32)
        v_more = jnp.dot(normed[:, columns], wv[columns], preferred_element_type=F32)
        if steps == 0:
            k_sum[...] = k_more
            v_sum[...] = v_more
        elif steps != 2:
            k_sum[...] += k_more
            v_sum[...] += v_more
        else:
            k_all = k_sum[...] + k_more
            v_all = (v_sum[...] + v_more).astype(BF16)
    v_s[...] = v_all[:tokens]
    k_s[...] = rotated(k_all[:tokens], cos_s[...], sin_s[...], low).astype(BF16)
    ck = rotated(k_all[tokens:], ccos, csin, low).astype(BF16).astype(F32)
    cv = v_all[tokens:]
    spot = (sp * ctx_rows + lax.broadcasted_iota(jnp.int32, (ctx_rows, 1), 0)).astype(F32)
    cf = squeezed(outer(ck * jnp.exp(ldf * (ctx_len - 1.0 - spot)), cv), masks)
    cb = squeezed(outer(ck * jnp.exp(ldb * spot), cv), masks)
    l = lax.broadcasted_iota(jnp.int32, (BLOCK, 1), 0).astype(F32)
    to_end, to_start = jnp.exp(ldf * (BLOCK - 1.0 - l)), jnp.exp(ldb * l)
    gf, gb = jnp.exp(ldf * BLOCK), jnp.exp(ldb * BLOCK)
    sf = jnp.zeros((HEAD, width), F32)
    ub = []
    for b in range(blocks):
        keys = k_s[b * BLOCK : (b + 1) * BLOCK].astype(F32)
        values = v_s[b * BLOCK : (b + 1) * BLOCK]
        u_s[b] = sf
        sf = gf * sf + squeezed(outer(keys * to_end, values), masks)
        ub.append(squeezed(outer(keys * to_start, values), masks))
    sb = jnp.zeros((HEAD, width), F32)
    for b in reversed(range(blocks)):
        u_s[blocks + b] = sb
        sb = gb * sb + ub[b]
    for s in range(ny):
        rows = slice(s * part, (s + 1) * part)
        st[s] = jnp.concatenate([sf[rows], sb[rows], cf[rows], cb[rows]], axis=0).astype(BF16)
    one = Line(at, "sp_1", ny, a_send, a_recv)
    one.start(lambda there: st.at[there], r1)
    r1[y] = st[y]

    weights[2].wait()
    q_all = jnp.dot(normed[0:tokens], wq[...], preferred_element_type=F32)
    queries = (rotated(q_all, cos_s[...], sin_s[...], low) * HEAD ** (-0.5)).astype(BF16)
    read_f, read_b = jnp.exp(ldf * (l + 1.0)), jnp.exp(ldb * (BLOCK - l))
    a = lax.broadcasted_iota(jnp.int32, (width, width), 0)
    b = lax.broadcasted_iota(jnp.int32, (width, width), 1)
    average = jnp.where(a // HEAD == b // HEAD, 1.0 / HEAD, 0.0).astype(BF16)
    q_s[...] = queries

    def near(i):
        rows = slice(i * BLOCK, (i + 1) * BLOCK)
        wide = q_s[rows].astype(F32)
        stacked = jnp.concatenate([jnp.where(m, wide, 0.0) for m in masks], axis=0).astype(BF16)
        scores = lax.dot_general(
            stacked, k_s[rows], (((1,), (1,)), ((), ())), preferred_element_type=F32
        )
        inside = jnp.dot(
            (scores * decay[...]).astype(BF16), v_s[rows], preferred_element_type=F32
        )
        states = jnp.concatenate(
            [spread_out(u_s[i], masks), spread_out(u_s[blocks + i], masks)], axis=0
        ).astype(BF16)
        near_f, near_b = wide * read_f, wide * read_b
        o = jnp.dot(
            jnp.concatenate([near_f, near_b], axis=1).astype(BF16), states,
            preferred_element_type=F32,
        )
        for h, m in enumerate(masks):
            o = o + jnp.where(m, inside[h * BLOCK : (h + 1) * BLOCK], 0.0)
        o_s[rows] = o - averaged(o, average)
        far_f = wide * jnp.exp(ldf * (l + (i * BLOCK + 1.0)))
        far_b = wide * jnp.exp(ldb * ((tokens - i * BLOCK) - l))
        readers[rows] = jnp.concatenate([far_f, far_b], axis=1).astype(BF16)

    for i in range(blocks // 2):
        near(i)
    span = float(tokens * ny)
    factors = []
    for k in range(nz):
        there = lax.rem(z + k, nz)
        ahead_by = (there - z).astype(F32)
        to_f = jnp.where(there > z, 1.0, 0.0) * jnp.exp(ldf * (span * jnp.maximum(ahead_by - 1.0, 0.0)))
        to_b = jnp.where(there < z, 1.0, 0.0) * jnp.exp(ldb * (span * jnp.maximum(-ahead_by - 1.0, 0.0)))
        start_f = jnp.exp(ldf * (span * there.astype(F32)))
        start_b = jnp.exp(ldb * (span * (nz - 1 - there).astype(F32)))
        factors.append((there, to_f, to_b, start_f, start_b))
    one.wait(r1)
    got = [r1[j].astype(F32) for j in range(ny)]
    hf, hb = jnp.exp(ldf * tokens), jnp.exp(ldb * tokens)
    ahead = [jnp.zeros_like(got[0][:part])]
    for j in range(ny):
        ahead.append(hf * ahead[-1] + got[j][:part])
    total_f = ahead.pop()
    behind = [jnp.zeros_like(ahead[0])]
    for j in reversed(range(ny)):
        behind.append(hb * behind[-1] + got[j][part : 2 * part])
    total_b = behind.pop()
    behind = behind[::-1]
    ctx = sum(got)
    ctx_f, ctx_b = ctx[2 * part : 3 * part], ctx[3 * part :]
    for there, to_f, to_b, start_f, start_b in factors:
        s2[there] = jnp.concatenate(
            [to_f * total_f + start_f * ctx_f, to_b * total_b + start_b * ctx_b], axis=0
        ).astype(BF16)
    two = Line(at, "sp_0", nz, b_send, b_recv)
    two.start(lambda there: s2.at[there], r2)
    r2[z] = s2[z]
    for i in range(blocks // 2, blocks):
        near(i)
    wc.wait(w_yz)
    two.wait(r2)
    entering = sum(r2[j].astype(F32) for j in range(nz))
    for j in range(ny):
        s3[j] = jnp.concatenate(
            [
                ahead[j] + jnp.exp(ldf * float(tokens * j)) * entering[:part],
                behind[j] + jnp.exp(ldb * float(tokens * (ny - 1 - j))) * entering[part:],
            ],
            axis=0,
        ).astype(BF16)
    three = Line(at, "sp_1", ny, c_send, c_recv)
    three.start(lambda there: s3.at[there], ent)
    ent[y] = s3[y]
    wd.wait(w_zy)
    for a in range(nz):
        for b in range(ny):
            first = (a * ny + b) * wrows
            wall[core, first : first + wrows, 0:128] = w_yz[a, b]
            wall[core, first : first + wrows, 128:256] = w_zy[b, a]
    over = {"tp_1": 1 - core}
    w_over = remote(wall.at[core], wall.at[core], x_send.at[0], x_recv.at[0], over)
    w_over.start()
    three.wait(ent)

    slices = [ent[s].astype(F32) for s in range(ny)]
    packed = jnp.concatenate([e[:part] for e in slices] + [e[part:] for e in slices], axis=0)
    packed = packed - averaged(packed, average)
    states = jnp.concatenate(
        [spread_out(packed[:HEAD], masks), spread_out(packed[HEAD:], masks)], axis=0
    ).astype(BF16)
    order = (2, 1, 3, 0)
    right, left = lax.rem(x + 1, nx), lax.rem(x + nx - 1, nx)
    to_right, to_left = {"tp_0": right}, {"tp_0": left}
    partner = t + 1 - 2 * core
    posted = []

    def post(src, dst, q, s, r, device):
        copy = remote(src, dst, g_send.at[q, s], g_recv.at[q, r], device)
        copy.start()
        posted.append(copy)

    def arrived(q, s, r):
        remote(
            gathered.at[q, s], gathered.at[q, s], g_send.at[q, 0], g_recv.at[q, r], over
        ).wait_recv()

    for steps in order:
        q = lax.rem(x + steps, nx)
        rows = pl.ds(pl.multiple_of(q * 2 * own, 2 * own), 2 * own)
        centred = o_s[rows] + jnp.dot(readers[rows], states, preferred_element_type=F32)
        spread = jnp.dot((centred * centred).astype(BF16), average, preferred_element_type=F32)
        kept = (centred * lax.rsqrt(spread + EPSILON) * hg_ref[...]).astype(BF16)
        ret[2 * q] = kept[:own]
        ret[2 * q + 1] = kept[own:]
        post(ret.at[2 * q + 1 - core], gathered.at[q, t], q, 0, 0, over)
        post(ret.at[2 * q + core], gathered.at[q, t], q, 1, 1 + core, to_right)
        post(ret.at[2 * q + core], gathered.at[q, t], q, 2, 3 + core, to_left)
        gathered[q, t] = ret[2 * q + core]
    for steps in order:
        q = lax.rem(x + steps, nx)
        arrived(q, partner, 0)
        post(gathered.at[q, partner], gathered.at[q, partner], q, 3, 2 - core, to_right)
        post(gathered.at[q, partner], gathered.at[q, partner], q, 4, 4 - core, to_left)
    for steps in order:
        q = lax.rem(left + steps, nx)
        arrived(q, 2 * left, 1)
        post(gathered.at[q, 2 * left], gathered.at[q, 2 * left], q, 5, 5, to_right)
        q = lax.rem(right + steps, nx)
        arrived(q, 2 * right + 1, 4)
        post(gathered.at[q, 2 * right + 1], gathered.at[q, 2 * right + 1], q, 6, 6, to_left)
    w_over.wait_recv()
    far = lax.rem(x + 2, nx)

    qs = [lax.rem(x + steps, nx) for steps in order]

    def block(q, chip):
        return jnp.concatenate([gathered[q, 2 * chip], gathered[q, 2 * chip + 1]], axis=1)

    def matrix(k, chip):
        return wall[k, pl.ds(pl.multiple_of(chip * 2 * width, 2 * width), 2 * width)]

    for q in qs:
        arrived(q, 2 * left + 1, 2)
        arrived(q, 2 * right, 3)
    for k in range(2):
        near_sum[:, k * width : (k + 1) * width] = sum(
            jnp.dot(
                jnp.concatenate([block(q, chip) for q in qs], axis=0), matrix(k, chip),
                preferred_element_type=F32,
            )
            for chip in (x, left, right)
        )

    def finish(spots):
        for i in spots:
            arrived(qs[i], 2 * far, 5)
            arrived(qs[i], 2 * far + 1, 6)
        rows = jnp.concatenate([block(qs[i], far) for i in spots], axis=0)
        for k in range(2):
            columns = pl.ds(pl.multiple_of((2 * x + k) * width, width), width)
            more = jnp.dot(rows, matrix(k, far), preferred_element_type=F32)
            for j, i in enumerate(spots):
                q = qs[i]
                mine = pl.ds(pl.multiple_of((2 * q + core) * own, own), own)
                mixed = near_sum[i * own : (i + 1) * own, k * width : (k + 1) * width]
                mixed = mixed + more[j * own : (j + 1) * own]
                result = rows_all[mine, columns].astype(F32) + mod[2:3, columns] * mixed
                done[q, k] = result.astype(BF16)
                if order[i]:
                    copy = remote(
                        done.at[q, k], landed.at[x, k], o_send.at[i, k], o_recv.at[x, k],
                        {"tp_0": q},
                    )
                    copy.start()
                    posted.append(copy)

    finish([0])
    finish([1, 2])
    finish([3])
    landed[x] = done[x]
    for chip in (right, left, far):
        for k in range(2):
            view = landed.at[chip, k]
            remote(view, view, o_send.at[0, k], o_recv.at[chip, k], {"tp_0": chip}).wait_recv()
    for chip in range(nx):
        for k in range(2):
            first = (chip * 2 + k) * width
            out_ref[:, first : first + width] = landed[chip, k]
    for line in (along_y, along_z, wa, wb, wc, wd, one, two, three, spread_rows):
        line.drain()
    for copy in sent + posted + [w_over]:
        copy.wait_send()


def turns(positions):
    frequency = ROTARY_BASE ** -np.linspace(0.0, 1.0, HALF)
    angles = np.asarray(positions, np.float64)[:, None] * frequency[None]
    tile = lambda a: np.tile(np.asarray(a, np.float32), (1, 128 // HALF))
    return tile(np.cos(angles)), tile(np.sin(angles))


def per_device(
    sizes, latent, context, condition, context_condition, modulation_weight, norm_gain,
    query_weight, key_weight, value_weight, log_decay, head_gain, output_weight,
):
    ny, nz, nx = sizes
    nt = 2 * nx
    d = latent.shape[1]
    width = query_weight.shape[1]
    heads = width // HEAD
    own = latent.shape[0]
    tokens = own * nt
    ctx_rows = context.shape[0]
    ctx_len = ctx_rows * ny * nz
    wrows = output_weight.shape[0]
    cos_off, sin_off = turns(np.arange(tokens))
    bases = np.stack(
        turns(ctx_len + tokens * np.arange(ny * nz)) + turns(ctx_rows * np.arange(ny * nz)), axis=1
    )
    ins = [
        condition.reshape(1, d), context_condition.reshape(1, d),
        modulation_weight.transpose(1, 0, 2), latent, context, output_weight, norm_gain.reshape(1, d),
        log_decay, head_gain.reshape(1, width), jnp.asarray(cos_off), jnp.asarray(sin_off),
        jnp.asarray(bases), query_weight, key_weight, value_weight,
    ]
    dma = lambda *n: pltpu.SemaphoreType.DMA(n)
    part, blocks = HEAD // ny, tokens // BLOCK
    pair = lambda n: [dma(n), dma(n)]
    scratch = [
        pltpu.VMEM(shape, kind)
        for shape, kind in (
            ((tokens, 128), F32), ((tokens, 128), F32), ((4, 128), F32),
            *[((d, width), BF16)] * 3,
            ((8, width), F32), ((8, d), F32), ((tokens, d), BF16), ((tokens, 128), F32),
            ((tokens + ctx_rows, d), BF16), ((tokens, width), F32), ((tokens, width), F32),
            ((heads * BLOCK, BLOCK), F32),
            ((ny, 8, width), F32), ((nz, 8, width), F32), ((nt, 8, width), F32),
            ((8, width), F32), ((8, width), F32),
            ((nz, ny, wrows, 128), BF16), ((ny, nz, wrows, 128), BF16), ((2, d, width), BF16),
            ((tokens + ctx_rows, width), F32), ((tokens + ctx_rows, width), F32),
            ((tokens, width), BF16), ((tokens, width), BF16), ((tokens, width), BF16),
            ((2 * blocks, HEAD, width), F32),
            ((tokens, width), F32), ((tokens, 2 * width), BF16),
            ((ny, 4 * part, width), BF16), ((ny, 4 * part, width), BF16),
            ((nz, 2 * part, width), BF16), ((nz, 2 * part, width), BF16),
            ((ny, 2 * part, width), BF16), ((ny, 2 * part, width), BF16),
            ((nt, own, width), BF16), ((nx, nt, own, width), BF16),
            ((nx * own, 2 * width), F32),
            ((nx, 2, own, width), BF16), ((nx, 2, own, width), BF16),
        )
    ] + [
        dma(6), *pair(ny), *pair(nz), *pair(nt), *pair(GATHER_SEMS),
        *pair(ny), *pair(nz), *pair(nz), *pair(ny),
        *pair(ny), *pair(nz), *pair(ny), dma(nx, 7), dma(nx, 7), dma(nx, 2), dma(nx, 2), *pair(1),
    ]
    near = pl.BlockSpec(memory_space=pltpu.VMEM)
    return pl.pallas_call(
        functools.partial(whole_kernel, sizes, ctx_len),
        out_shape=pltpu.VMEM((own, d), BF16),
        in_specs=[near] * (len(ins) - 6) + [pl.BlockSpec(memory_space=pl.ANY)] * 6,
        out_specs=near,
        scratch_shapes=scratch,
        compiler_params=pltpu.CompilerParams(
            vmem_limit_bytes=VMEM_LIMIT, collective_id=0, has_side_effects=True
        ),
    )(*ins)


def solution(mesh, ny=8, nz=8, nx=4):
    split = Mesh(mesh.devices.reshape(nz, ny, nx, 2), SP_TP)
    placed = (
        P(SP_TP, None), P(SP, None), P(), P(), P(SP, None, TP), P(), P(None, TP), P(None, TP),
        P(None, TP), P(None, TP), P(TP), P(SP, None),
    )
    return jax.shard_map(
        functools.partial(per_device, (ny, nz, nx)), mesh=split, in_specs=placed,
        out_specs=P(SP_TP, None), check_vma=False,
    )
```
